1024 devices in a mesh: row: 64 (over z, y), col: 16 (over x, core).
Axes of the slice: x: 8, y: 8, z: 8, core: 2. Of those that a mesh axis runs over, the one named last changes fastest.
Arguments:
- tokens: bfloat16 [32768, 2048], P('row'), may hold values from -6 to 6
- outer_weight: bfloat16 [2048, 1024], P(None, 'col'), may hold values from -0.125 to 0.125
- inner_weight: bfloat16 [2048, 1024], P(None, 'col'), may hold values from -0.125 to 0.125
- value_weight: bfloat16 [2048, 1024], P(None, 'col'), may hold values from -0.125 to 0.125
- conv_taps: float32 [3, 3, 1024], P(None, None, 'col'), may hold values from -3.5 to 3.5
- feature_weight: float32 [33, 128], replicated, may hold values from -1 to 1
- feature_phase: float32 [128], replicated, may hold values from -3.140625 to 3.140625
- inner_mats: float32 [2, 128, 128], replicated, may hold values from -0.5 to 0.5
- inner_phase: float32 [2, 128], replicated, may hold values from -3.140625 to 3.140625
- frequency: float32 [128], replicated, may hold values from 0.1 to 1.9
- forward_weight: float32 [128, 1024], P(None, 'col'), may hold values from -0.5 to 0.5
- backward_weight: float32 [128, 1024], P(None, 'col'), may hold values from -0.5 to 0.5
- decay_rate: float32 [1024], P('col'), may hold values from 0.2 to 3276.8, as said below
- skip_gain: float32 [1024], P('col'), may hold values from -6 to 6
- output_weight: bfloat16 [1024, 2048], replicated, may hold values from -0.1875 to 0.1875
Outputs:
- layer_out: bfloat16 [32768, 2048], P(('row', 'col'))
The draws below stay inside these ranges and needn't reach their ends.
Inputs may be any that keep to these rules, and one draw needn't show every extreme that they name: `decay_rate`: positive rates of the channels' filter windows.
All inputs are finite; a program needn't handle non-finite values.
Results may differ from the reference program's by a relative error of at most 0.014.
Values may be sent and summed in bfloat16 or wider, within the bound.
A program may use at most 64 MiB of HBM per device.

```python
import math
import jax
import jax.numpy as jnp
from jax import lax

D = 2048
C = 1024
UNITS = 128
BANDS = 16
INNER = 2
LENGTH = 32768


def draw_decay_rate(key, part):
    picker, slow_key, fast_key = jax.random.split(key, 3)
    share = 0.5
    fast_mask = jax.random.uniform(picker, (C,), jnp.float32) < share
    slow_rate = jax.random.uniform(slow_key, (C,), jnp.float32, 0.2, 2.0)
    fast_rate = LENGTH / jax.random.uniform(fast_key, (C,), jnp.float32, 10.0, 30.0)
    return jnp.where(fast_mask, fast_rate, slow_rate).astype(jnp.float32)


def block_scale(own_key, shape, shards, least, largest):
    gain = 1.0
    for position, parts in shards:
        heights = jax.random.uniform(jax.random.fold_in(jax.random.fold_in(own_key, 6), position), (parts,), jnp.float32, least / len(shards), largest / len(shards))
        gain = gain * jnp.repeat(jnp.exp(heights), shape[position] // parts).reshape((-1,) + (1,) * (len(shape) - 1 - position))
    return gain


def centred(own_key, shape, width, limit, cuts=(), kind=jnp.bfloat16):
    values = jax.random.normal(own_key, shape, jnp.float32) * width
    if len(cuts) > 0:
        values = block_scale(own_key, shape, cuts, -0.22, 0.18) * values
    return jnp.clip(values, min=-limit, max=limit).astype(kind)


def setup_inputs(seed: int = 0) -> dict:
    arg_keys = jax.random.split(jax.random.key(seed), 16)
    tokens = centred(arg_keys[0], (LENGTH, D), 1.0, 6.0, ((0, 64),))
    outer_weight = centred(arg_keys[1], (D, C), D ** -0.5, 0.125, ((1, 16),))
    inner_weight = centred(arg_keys[2], (D, C), D ** -0.5, 0.125, ((1, 16),))
    value_weight = centred(arg_keys[3], (D, C), D ** -0.5, 0.125, ((1, 16),))
    conv_taps = centred(arg_keys[4], (3, 3, C), 0.577, 3.5, ((2, 16),), jnp.float32)
    feature_weight = centred(arg_keys[5], (2 * BANDS + 1, UNITS), (2 * BANDS + 1) ** -0.5, 1.0, (), jnp.float32)
    feature_phase = jnp.clip(jax.random.uniform(arg_keys[6], (UNITS,), jnp.float32, -3.140625, 3.140625), -3.140625, 3.140625)
    inner_mats = centred(arg_keys[7], (INNER, UNITS, UNITS), UNITS ** -0.5, 0.5, (), jnp.float32)
    inner_phase = jnp.clip(jax.random.uniform(arg_keys[8], (INNER, UNITS), jnp.float32, -3.140625, 3.140625), -3.140625, 3.140625)
    frequency = jnp.clip(1.0 + 0.18 * jax.random.normal(arg_keys[9], (UNITS,), jnp.float32), 0.1, 1.9)
    forward_weight = centred(arg_keys[10], (UNITS, C), UNITS ** -0.5, 0.5, ((1, 16),), jnp.float32)
    backward_weight = centred(arg_keys[11], (UNITS, C), UNITS ** -0.5, 0.5, ((1, 16),), jnp.float32)
    decay_rate = draw_decay_rate(jax.random.fold_in(arg_keys[15], 71), 0)
    skip_gain = centred(arg_keys[13], (C,), 1.0, 6.0, ((0, 16),), jnp.float32)
    output_weight = centred(arg_keys[14], (C, D), C ** -0.5, 0.1875)
    return {"tokens": tokens, "outer_weight": outer_weight, "inner_weight": inner_weight, "value_weight": value_weight, "conv_taps": conv_taps, "feature_weight": feature_weight, "feature_phase": feature_phase, "inner_mats": inner_mats, "inner_phase": inner_phase, "frequency": frequency, "forward_weight": forward_weight, "backward_weight": backward_weight, "decay_rate": decay_rate, "skip_gain": skip_gain, "output_weight": output_weight}


PRECISE = lax.Precision.HIGHEST

def short_conv(projected, tap_rows):
    padded = jnp.pad(projected.astype(jnp.float32), ((1, 1), (0, 0)))
    return padded[:-2] * tap_rows[0] + padded[1:-1] * tap_rows[1] + padded[2:] * tap_rows[2]

def reference(tokens, outer_weight, inner_weight, value_weight, conv_taps, feature_weight, feature_phase, inner_mats, inner_phase, frequency, forward_weight, backward_weight, decay_rate, skip_gain, output_weight):
    outer_proj = jnp.dot(tokens, outer_weight, preferred_element_type=jnp.float32).astype(jnp.bfloat16)
    inner_proj = jnp.dot(tokens, inner_weight, preferred_element_type=jnp.float32).astype(jnp.bfloat16)
    value_proj = jnp.dot(tokens, value_weight, preferred_element_type=jnp.float32).astype(jnp.bfloat16)
    places = jnp.arange(LENGTH, dtype=jnp.int32)
    scaled = places.astype(jnp.float32) / (LENGTH - 1)
    band_ints = 1 + jnp.arange(BANDS, dtype=jnp.int32) * (LENGTH // (4 * BANDS))
    turns = places[:, None] * band_ints[None, :] % LENGTH
    angles = 2.0 * math.pi / LENGTH * turns.astype(jnp.float32)
    features = jnp.concatenate([scaled[:, None], jnp.cos(angles), -jnp.sin(angles)], axis=1)
    hidden = jnp.sin(frequency * (jnp.dot(features, feature_weight, precision=PRECISE) + feature_phase))
    for level_index in range(INNER):
        hidden = jnp.sin(frequency * (jnp.dot(hidden, inner_mats[level_index], precision=PRECISE) + inner_phase[level_index]))
    channel_block = 128
    block_count = C // channel_block

    def split_cols(matrix):
        return matrix.reshape(matrix.shape[0], block_count, channel_block).transpose(1, 0, 2)

    def one_block(pieces):
        outer_part, inner_part, value_part, tap_block, ahead_cols, behind_cols, rates, skips = pieces
        gate_part = short_conv(outer_part, tap_block[:, 0]).astype(jnp.bfloat16)
        signal = (short_conv(inner_part, tap_block[:, 1]) * short_conv(value_part, tap_block[:, 2])).astype(jnp.bfloat16)
        window = jnp.exp(-scaled[:, None] * rates[None, :])
        filter_ahead = jnp.dot(hidden, ahead_cols, precision=PRECISE) * window
        filter_behind = jnp.dot(hidden, behind_cols, precision=PRECISE) * window
        norm_scale = lax.rsqrt(1.0 + lax.optimization_barrier(jnp.sum(jnp.square(filter_ahead), axis=0)) + lax.optimization_barrier(jnp.sum(jnp.square(filter_behind[1:]), axis=0)))
        kernel = jnp.concatenate([filter_ahead, jnp.zeros((1, channel_block), jnp.float32), filter_behind[:0:-1]], axis=0) * norm_scale
        signal_wide = signal.astype(jnp.float32)
        spectrum = jnp.fft.rfft(signal_wide, n=2 * LENGTH, axis=0) * jnp.fft.rfft(kernel, axis=0)
        response = jnp.fft.irfft(spectrum, n=2 * LENGTH, axis=0)[:LENGTH].astype(jnp.bfloat16)
        response = lax.optimization_barrier(response)
        return (gate_part.astype(jnp.float32) * (response.astype(jnp.float32) + skips * signal_wide)).astype(jnp.bfloat16)
    taps_split = conv_taps.reshape(3, 3, block_count, channel_block).transpose(2, 0, 1, 3)
    mixed_blocks = lax.map(one_block, (split_cols(outer_proj), split_cols(inner_proj), split_cols(value_proj), taps_split, split_cols(forward_weight), split_cols(backward_weight), decay_rate.reshape(block_count, channel_block), skip_gain.reshape(block_count, channel_block)))
    mixed_rows = mixed_blocks.transpose(1, 0, 2).reshape(LENGTH, C)
    return jnp.dot(mixed_rows, output_weight, preferred_element_type=jnp.float32).astype(jnp.bfloat16)
```

```python
import functools
import math

import jax
import jax.numpy as jnp
import numpy as np
from jax import lax
from jax.experimental import pallas as pl
from jax.experimental.pallas import tpu as pltpu
from jax.sharding import PartitionSpec as P

BANDS = 16
INNER = 2
LANES = 128
MESH = pl.DeviceIdType.MESH
PRECISE = lax.Precision.HIGHEST
F32 = jnp.float32
BF16 = jnp.bfloat16


def tables(row_blocks):
    total = 2 * row_blocks * LANES
    k = np.arange(row_blocks)
    r = np.arange(row_blocks)
    b = np.arange(LANES)
    outer = (np.outer(2 * k + 1, r) % (4 * row_blocks)) * (2.0 * math.pi / (4 * row_blocks))
    one = np.concatenate([np.cos(outer), np.sin(outer)], axis=0)
    one_back = np.concatenate([np.cos(outer).T, -np.sin(outer).T], axis=1)
    inner = (np.outer(b, b) % LANES) * (2.0 * math.pi / LANES)
    c, s = np.cos(inner), np.sin(inner)
    two = np.block([[c, -s], [s, c]])
    two_back = np.block([[c, s], [-s, c]])
    twist = np.outer(2 * k + 1, b) * (math.pi / total)
    return (
        jnp.asarray(one, BF16),
        jnp.asarray(one_back, BF16),
        jnp.asarray(two, BF16),
        jnp.asarray(two_back, BF16),
        jnp.asarray(np.stack([np.cos(twist), np.sin(twist)]), F32),
    )


def mm(a, b):
    return jnp.dot(a, b, preferred_element_type=F32)


def kernel(rows, cols, seq_length, *refs):
    (
        tokens, outer_w, inner_w, value_w, taps_h, first_h, phase_h, mats_h, iphase_h, freq_h,
        ahead_h, behind_h, rate_h, skip_h, map_h, one_h, one_back_h, two_h, two_back_h, twist_h,
        out_ref,
        tok, w_o, w_i, w_v, taps, first, phase, mats, iphase, freq, ahead_w, behind_w, rate, skip,
        out_w, one, one_back, two, two_back, twist,
        proj, gate_s, sig_s, f_send, f_recv, s_send, s_recv, y_send, y_recv, m_send, m_recv,
        load_sem, halo_send, halo_recv, a2a_send, a2a_recv,
    ) = refs
    me_r, me_c = lax.axis_index("row"), lax.axis_index("col")
    length = tok.shape[0]
    width = w_o.shape[1]
    subs = length // LANES
    chunks = 4
    step = length // chunks

    def load(src, dst, index):
        copy = pltpu.make_async_copy(src, dst, load_sem.at[index])
        copy.start()
        return copy

    small = [
        load(s, d, i)
        for i, (s, d) in enumerate(
            [
                (first_h, first), (phase_h, phase), (mats_h, mats), (iphase_h, iphase), (freq_h, freq),
                (ahead_h, ahead_w), (behind_h, behind_w), (rate_h, rate),
            ]
        )
    ]
    weights = [load(s, d, 8 + i) for i, (s, d) in enumerate([(inner_w, w_i), (outer_w, w_o), (value_w, w_v)])]
    token_loads = [
        load(tokens.at[pl.ds(c * step, step)], tok.at[pl.ds(c * step, step)], 11 + c) for c in range(chunks)
    ]

    barrier = pltpu.get_barrier_semaphore()

    def greet_row(d, carry):
        peer = lax.rem(me_r + d, rows)
        pl.semaphore_signal(barrier, inc=1, device_id=(peer, me_c), device_id_type=MESH)
        return carry

    def greet_col(d, carry):
        peer = lax.rem(me_c + d, cols)
        pl.semaphore_signal(barrier, inc=1, device_id=(me_r, peer), device_id_type=MESH)
        return carry

    lax.fori_loop(1, rows, greet_row, 0)
    lax.fori_loop(1, cols, greet_col, 0)

    for copy in small:
        copy.wait()
    place = me_r * length + lax.broadcasted_iota(jnp.int32, (length, LANES), 0)
    lane = lax.broadcasted_iota(jnp.int32, (length, LANES), 1)
    is_sine = lane > BANDS
    band = 1 + jnp.where(is_sine, lane - (BANDS + 1), lane - 1) * (seq_length // (4 * BANDS))
    turns = (place * band + jnp.where(is_sine, seq_length // 4, 0)) & (seq_length - 1)
    waves = jnp.cos(2.0 * math.pi / seq_length * turns.astype(F32))
    scaled = place.astype(F32) / (seq_length - 1)
    features = jnp.where(lane == 0, scaled, waves)[:, : 2 * BANDS + 1]
    hidden = jnp.sin(freq[...] * (jnp.dot(features, first[...], precision=PRECISE, preferred_element_type=F32) + phase[...]))
    for level in range(INNER):
        hidden = jnp.sin(
            freq[...]
            * (jnp.dot(hidden, mats[level], precision=PRECISE, preferred_element_type=F32) + iphase[level : level + 1, :])
        )
    both = jnp.concatenate([ahead_w[...], behind_w[...]], axis=1)
    rates = jnp.concatenate([rate[...], rate[...]], axis=1)
    filters = jnp.dot(hidden, both, precision=PRECISE, preferred_element_type=F32) * jnp.exp(
        -scaled[:, : 2 * width] * rates
    )
    filters = jnp.where((place[:, : 2 * width] == 0) & (lane[:, : 2 * width] >= width), 0.0, filters)
    turned = filters.T
    fa, fb = turned[:width], turned[width:]
    f_send[...] = jnp.concatenate([fa + fb, fa - fb], axis=1).reshape(width, 2 * subs, LANES).astype(BF16)

    for copy in weights:
        copy.wait()
    joined = jnp.concatenate([w_i[...], w_o[...], w_v[...]], axis=1)
    for c in range(chunks):
        token_loads[c].wait()
        part = mm(tok[pl.ds(c * step, step), :], joined)
        proj[pl.ds(8 + c * step, step), :] = part.astype(BF16).astype(F32)

    late = [
        load(s, d, 11 + chunks + i)
        for i, (s, d) in enumerate(
            [
                (taps_h, taps), (skip_h, skip), (one_h, one), (two_h, two), (twist_h, twist),
                (two_back_h, two_back), (one_back_h, one_back), (map_h, out_w),
            ]
        )
    ]

    pl.semaphore_wait(barrier, rows + cols - 2)

    after, before = lax.rem(me_r + 1, rows), lax.rem(me_r + rows - 1, rows)
    up = pltpu.make_async_remote_copy(
        proj.at[pl.ds(length, 8)], proj.at[pl.ds(0, 8)], halo_send.at[0], halo_recv.at[0],
        device_id=(after, me_c), device_id_type=MESH,
    )
    down = pltpu.make_async_remote_copy(
        proj.at[pl.ds(8, 8)], proj.at[pl.ds(8 + length, 8)], halo_send.at[1], halo_recv.at[1],
        device_id=(before, me_c), device_id_type=MESH,
    )
    up.start()
    down.start()

    def scatter(send, recv, index):
        def one_peer(d, carry):
            peer = lax.rem(me_r + d, rows)
            pltpu.make_async_remote_copy(
                send.at[peer], recv.at[me_r], a2a_send.at[index], a2a_recv.at[index],
                device_id=(peer, me_c), device_id_type=MESH,
            ).start()
            return carry

        lax.fori_loop(1, rows, one_peer, 0)
        recv[me_r] = send[me_r]

    def drain(ref, count, sem):
        pltpu.make_async_copy(ref.at[pl.ds(0, count)], ref.at[pl.ds(0, count)], sem).wait()

    scatter(f_send, f_recv, 0)

    for copy in late[:2]:
        copy.wait()
    up.wait()
    down.wait()
    proj[7:8, :] = jnp.where(me_r == 0, 0.0, proj[7:8, :])
    proj[8 + length : 9 + length, :] = jnp.where(me_r == rows - 1, 0.0, proj[8 + length : 9 + length, :])
    tap = [
        jnp.concatenate([taps[a, 1:2, :], taps[a, 0:1, :], taps[a, 2:3, :]], axis=1) for a in range(3)
    ]
    conv = proj[7 : 7 + length, :] * tap[0] + proj[8 : 8 + length, :] * tap[1] + proj[9 : 9 + length, :] * tap[2]
    signal = (conv[:, :width] * conv[:, 2 * width :]).astype(BF16).astype(F32)
    gate_s[...] = conv[:, width : 2 * width].astype(BF16).astype(F32)
    sig_s[...] = signal
    s_send[...] = signal.T.reshape(width, subs, LANES).astype(BF16)
    scatter(s_send, s_recv, 1)

    half = rows * subs
    for copy in late[2:5]:
        copy.wait()
    twist_c, twist_s = twist[0], twist[1]

    def first_stage(x):
        turned = mm(one[...], x)
        real, imag = turned[:half], turned[half:]
        return jnp.concatenate(
            [real * twist_c - imag * twist_s, -(imag * twist_c + real * twist_s)], axis=1
        ).astype(BF16)

    drain(f_recv, rows - 1, a2a_recv.at[0])
    got = f_recv[...].astype(F32)
    plus = got[:, :subs].reshape(half, LANES)
    minus = got[:, subs:].reshape(half, LANES)
    energy = jnp.sum(plus * plus + minus * minus, axis=0, keepdims=True)
    scale = lax.rsqrt(1.0 + 0.5 * jnp.sum(energy, axis=1, keepdims=True)) * (1.0 / (half * LANES))
    spec_real = mm(first_stage(plus.astype(BF16)), two[:, :LANES]) * scale
    spec_imag = mm(first_stage(minus.astype(BF16)), two[:, LANES:]) * scale

    for copy in late[5:7]:
        copy.wait()
    drain(s_recv, rows - 1, a2a_recv.at[1])
    spec = mm(first_stage(s_recv[...].astype(F32).reshape(half, LANES).astype(BF16)), two[...])
    real, imag = spec[:, :LANES], spec[:, LANES:]
    product = jnp.concatenate(
        [real * spec_real - imag * spec_imag, real * spec_imag + imag * spec_real], axis=1
    ).astype(BF16)
    back = mm(product, two_back[...])
    real, imag = back[:, :LANES], back[:, LANES:]
    untwisted = jnp.concatenate(
        [real * twist_c - imag * twist_s, imag * twist_c + real * twist_s], axis=0
    ).astype(BF16)
    response = mm(one_back[...], untwisted)
    y_send[...] = response.reshape(rows, subs, LANES).astype(BF16)
    scatter(y_send, y_recv, 2)

    skipped = skip[...] * sig_s[...]
    drain(y_recv, rows - 1, a2a_recv.at[2])
    replied = y_recv[...].astype(F32).reshape(width, length).T
    mixed = (gate_s[...] * (replied + skipped)).astype(BF16)
    m_send[...] = mixed.reshape(cols, length // cols, width)

    def col_peer(d, carry):
        peer = lax.rem(me_c + d, cols)
        pltpu.make_async_remote_copy(
            m_send.at[peer], m_recv.at[me_c], a2a_send.at[3], a2a_recv.at[3],
            device_id=(me_r, peer), device_id_type=MESH,
        ).start()
        return carry

    lax.fori_loop(1, cols, col_peer, 0)
    m_recv[me_c] = m_send[me_c]
    late[7].wait()
    drain(m_recv, cols - 1, a2a_recv.at[3])
    whole = jnp.concatenate([m_recv[j] for j in range(cols)], axis=1)
    tile = min(512, out_ref.shape[1])
    for c in range(out_ref.shape[1] // tile):
        out_ref[:, c * tile : (c + 1) * tile] = mm(whole, out_w[:, c * tile : (c + 1) * tile]).astype(BF16)

    drain(f_send, rows - 1, a2a_send.at[0])
    drain(s_send, rows - 1, a2a_send.at[1])
    drain(y_send, rows - 1, a2a_send.at[2])
    drain(m_send, cols - 1, a2a_send.at[3])


def on_device(rows, cols, *args):
    (
        tokens, outer_weight, inner_weight, value_weight, conv_taps, feature_weight, feature_phase, inner_mats,
        inner_phase, frequency, forward_weight, backward_weight, decay_rate, skip_gain, output_weight,
    ) = args
    length, model = tokens.shape
    width = outer_weight.shape[1]
    units = frequency.shape[0]
    subs = length // LANES
    seq_length = length * rows
    out_rows = length // cols
    operands = (
        tokens, outer_weight, inner_weight, value_weight, conv_taps, feature_weight, feature_phase.reshape(1, units),
        inner_mats, inner_phase, frequency.reshape(1, units), forward_weight, backward_weight,
        decay_rate.reshape(1, width), skip_gain.reshape(1, width), output_weight,
    ) + tables(rows * subs)
    slab = lambda n: pltpu.VMEM((rows, n, LANES), BF16)
    scratch = [pltpu.VMEM(x.shape, x.dtype) for x in operands] + [
        pltpu.VMEM((length + 16, 3 * width), F32),
        pltpu.VMEM((length, width), F32),
        pltpu.VMEM((length, width), F32),
        slab(2 * subs), slab(2 * subs), slab(subs), slab(subs), slab(subs), slab(subs),
        pltpu.VMEM((cols, out_rows, width), BF16),
        pltpu.VMEM((cols, out_rows, width), BF16),
        pltpu.SemaphoreType.DMA((24,)),
        pltpu.SemaphoreType.DMA((2,)),
        pltpu.SemaphoreType.DMA((2,)),
        pltpu.SemaphoreType.DMA((4,)),
        pltpu.SemaphoreType.DMA((4,)),
    ]
    return pl.pallas_call(
        functools.partial(kernel, rows, cols, seq_length),
        out_shape=jax.ShapeDtypeStruct((out_rows, model), BF16),
        in_specs=[pl.BlockSpec(memory_space=pl.ANY)] * len(operands),
        out_specs=pl.BlockSpec(memory_space=pltpu.VMEM),
        scratch_shapes=scratch,
        compiler_params=pltpu.CompilerParams(
            collective_id=0, has_side_effects=True, vmem_limit_bytes=56 * 1024 * 1024
        ),
    )(*operands)


def solution(mesh):
    placed = (
        P("row", None),
        P(None, "col"),
        P(None, "col"),
        P(None, "col"),
        P(None, None, "col"),
        P(),
        P(),
        P(),
        P(),
        P(),
        P(None, "col"),
        P(None, "col"),
        P("col"),
        P("col"),
        P(),
    )
    return jax.shard_map(
        functools.partial(on_device, mesh.shape["row"], mesh.shape["col"]),
        mesh=mesh, in_specs=placed, out_specs=P(("row", "col"), None), check_vma=False,
    )
```

```python
import functools
import math

import jax
import jax.numpy as jnp
import numpy as np
from jax import lax
from jax.experimental import pallas as pl
from jax.experimental.pallas import tpu as pltpu
from jax.sharding import PartitionSpec as P

BANDS = 16
INNER = 2
LANES = 128
MESH = pl.DeviceIdType.MESH
F32 = jnp.float32
BF16 = jnp.bfloat16


def tables(row_blocks):
    total = 2 * row_blocks * LANES
    k = np.arange(row_blocks)
    r = np.arange(row_blocks)
    b = np.arange(LANES)
    outer = (np.outer(2 * k + 1, r) % (4 * row_blocks)) * (2.0 * math.pi / (4 * row_blocks))
    one = np.concatenate([np.cos(outer), np.sin(outer)], axis=0)
    one_back = np.concatenate([np.cos(outer).T, -np.sin(outer).T], axis=1)
    inner = (np.outer(b, b) % LANES) * (2.0 * math.pi / LANES)
    c, s = np.cos(inner), np.sin(inner)
    two = np.block([[c, -s], [s, c]])
    two_back = np.block([[c, s], [-s, c]])
    twist = np.outer(2 * k + 1, b) * (math.pi / total)
    return (
        jnp.asarray(one, BF16),
        jnp.asarray(one_back, BF16),
        jnp.asarray(two, BF16),
        jnp.asarray(two_back, BF16),
        jnp.asarray(np.stack([np.cos(twist), np.sin(twist)]), F32),
    )


def mm(a, b):
    return jnp.dot(a, b, preferred_element_type=F32)


def mm_t(a, b):
    return lax.dot_general(a, b, (((1,), (1,)), ((), ())), preferred_element_type=F32)


def split(x):
    high = x.astype(BF16)
    return high, (x - high.astype(F32)).astype(BF16)


def sine_near(x):
    x = jnp.maximum(jnp.minimum(x, math.pi - x), -math.pi - x)
    y = x * x
    p = y * (2.6083159809786593e-6) - 1.9810690719168633e-4
    p = p * y + 8.333078585565090e-3
    p = p * y - 1.6666659712791443e-1
    return x + x * (y * p)


def sine(x):
    turns = jnp.round(x * (0.5 / math.pi))
    x = x - turns * 6.28125
    x = x - turns * 1.93500518798828125e-3
    x = x - turns * 3.0199159819567530e-7
    return sine_near(x)


def spread(i, size):
    return size // 2 + ((i + 1) // 2) * (1 - 2 * lax.rem(i, 2))


def kernel(rows, cols, seq_length, *refs):
    (
        tokens, outer_w, inner_w, value_w, taps_h, first_h, phase_h, mats_h, iphase_h, freq_h,
        ahead_h, behind_h, rate_h, skip_h, map_h, one_h, one_back_h, two_h, two_back_h, twist_h,
        out_ref,
        tok, w_all, taps, first, phase, mats, iphase, freq, both, rate, skip,
        out_w, one, one_back, two, two_back, twist,
        proj, gate_s, sig_s, f_send, f_recv, s_send, s_recv, y_send, y_recv, m_send, m_recv,
        load_sem, halo_send, halo_recv, a2a_send, a2a_recv,
    ) = refs
    me_r, me_c = lax.axis_index("row"), lax.axis_index("col")
    length = tok.shape[0]
    width = w_all.shape[0] // 3
    subs = length // LANES
    zone = rows // 2
    per = width // zone
    ring = 8 if rows % 8 == 0 else 2
    me_z, me_y = me_r // ring, lax.rem(me_r, ring)
    after, before = lax.rem(me_r + 1, rows), lax.rem(me_r + rows - 1, rows)
    in_zone = me_r < zone

    def load(src, dst, index):
        copy = pltpu.make_async_copy(src, dst, load_sem.at[index])
        copy.start()
        return copy

    small = [
        load(s, d, i)
        for i, (s, d) in enumerate(
            [
                (first_h, first), (phase_h, phase), (mats_h, mats), (iphase_h, iphase), (freq_h, freq),
                (ahead_h, both.at[pl.ds(0, width)]), (behind_h, both.at[pl.ds(width, width)]), (rate_h, rate),
            ]
        )
    ]
    weights = [load(w, w_all.at[pl.ds(i * width, width)], 8 + i) for i, w in enumerate((inner_w, value_w, outer_w))]
    token_load = load(tokens, tok, 11)

    barrier = pltpu.get_barrier_semaphore()

    def greet(row, col):
        pl.semaphore_signal(barrier, inc=1, device_id=(row, col), device_id_type=MESH)

    @pl.when(in_zone)
    def _():
        def greet_row(d, carry):
            greet(lax.rem(me_r + d, rows), me_c)
            return carry

        lax.fori_loop(1, rows, greet_row, 0)

    @pl.when(me_r >= zone)
    def _():
        greet(before, me_c)
        greet(after, me_c)

    def greet_col(i, carry):
        greet(me_r, lax.rem(me_c + spread(i, cols), cols))
        return carry

    lax.fori_loop(0, cols - 1, greet_col, 0)

    for copy in small:
        copy.wait()

    @pl.when(in_zone)
    def _():
        lane = lax.broadcasted_iota(jnp.int32, (length, LANES), 1)
        is_sine = lane > BANDS
        band = 1 + jnp.where(is_sine, lane - (BANDS + 1), lane - 1) * (seq_length // (4 * BANDS))
        shift = jnp.where(is_sine, seq_length, seq_length * 3 // 4)
        rates = jnp.broadcast_to(jnp.concatenate([rate[...], rate[...]], axis=1), (2 * width, 2 * width)).T[:, :1]
        behind = lax.broadcasted_iota(jnp.int32, (2 * width, length), 0) >= width
        w_first, w_mats, w_both = split(first[...]), split(mats[...]), split(both[...])

        def dot3(x, w, multiply):
            x_high, x_low = split(x)
            return multiply(x_high, w[0]) + (multiply(x_low, w[0]) + multiply(x_high, w[1]))

        for block in range(2):
            start = (me_r + block * zone) * length
            place = start + lax.broadcasted_iota(jnp.int32, (length, LANES), 0)
            turns = ((place * band + shift) & (seq_length - 1)) - seq_length // 2
            waves = sine_near(turns.astype(F32) * (2.0 * math.pi / seq_length))
            features = jnp.where(lane == 0, place.astype(F32) / (seq_length - 1), waves)[:, : 2 * BANDS + 1]
            hidden = sine(freq[...] * (dot3(features, w_first, mm) + phase[...]))
            for level in range(INNER):
                mat = (w_mats[0][level], w_mats[1][level])
                hidden = sine(freq[...] * (dot3(hidden, mat, mm) + iphase[level : level + 1, :]))
            turned = dot3(hidden, w_both, lambda h, w: mm_t(w, h))
            lag = start + lax.broadcasted_iota(jnp.int32, (2 * width, length), 1)
            turned = turned * jnp.exp(-(lag.astype(F32) / (seq_length - 1)) * rates)
            turned = jnp.where((lag == 0) & behind, 0.0, turned)
            fa, fb = turned[:width], turned[width:]
            f_send[block] = (
                jnp.concatenate([fa + fb, fa - fb], axis=1).reshape(width, 2 * subs, LANES).astype(BF16)
            )

    for copy in weights:
        copy.wait()
    token_load.wait()
    part = mm_t(tok[...], w_all[...]).astype(BF16)
    proj[pl.ds(8, length), :] = part.astype(F32)
    turned = part[:, : 2 * width].astype(F32).T
    s_send[...] = (
        jnp.concatenate([turned[:width], turned[width:]], axis=1).reshape(width, 2 * subs, LANES).astype(BF16)
    )

    outside = me_r // zone
    pl.semaphore_wait(barrier, zone - 1 + outside + before // zone + after // zone + cols - 1)

    def push(src, dst, index, row):
        pltpu.make_async_remote_copy(
            src, dst, a2a_send.at[index], a2a_recv.at[index], device_id=(row, me_c), device_id_type=MESH
        ).start()

    def drain(ref, count, sem):
        pltpu.make_async_copy(ref.at[pl.ds(0, count)], ref.at[pl.ds(0, count)], sem).wait()

    mine = pl.ds(per * me_r, per)
    zone_z = zone // ring

    def signal_peer(i, carry):
        peer = lax.rem(me_z + i, zone_z) * ring + lax.rem(me_y + spread(i // zone_z, ring), ring)

        @pl.when(peer != me_r)
        def _():
            push(s_send.at[pl.ds(per * peer, per)], s_recv.at[me_r], 1, peer)

        return carry

    lax.fori_loop(0, zone, signal_peer, 0)

    @pl.when(in_zone)
    def _():
        s_recv[me_r] = s_send[mine]

        def filter_peer(d, carry):
            peer = lax.rem(me_r + d, zone)
            push(f_send.at[0, pl.ds(per * peer, per)], f_recv.at[me_r], 0, peer)
            push(f_send.at[1, pl.ds(per * peer, per)], f_recv.at[me_r + zone], 0, peer)
            return carry

        lax.fori_loop(1, zone, filter_peer, 0)
        f_recv[me_r] = f_send[0, mine]
        f_recv[me_r + zone] = f_send[1, mine]

    late = [
        load(s, d, 12 + i)
        for i, (s, d) in enumerate(
            [
                (taps_h, taps), (skip_h, skip), (one_h, one), (two_h, two), (twist_h, twist),
                (two_back_h, two_back), (one_back_h, one_back), (map_h, out_w),
            ]
        )
    ]

    up = pltpu.make_async_remote_copy(
        proj.at[pl.ds(length, 8)], proj.at[pl.ds(0, 8)], halo_send.at[0], halo_recv.at[0],
        device_id=(after, me_c), device_id_type=MESH,
    )
    down = pltpu.make_async_remote_copy(
        proj.at[pl.ds(8, 8)], proj.at[pl.ds(8 + length, 8)], halo_send.at[1], halo_recv.at[1],
        device_id=(before, me_c), device_id_type=MESH,
    )
    up.start()
    down.start()
    for copy in late[:7]:
        copy.wait()

    half = rows * subs
    @pl.when(in_zone)
    def _():
        twist_c, twist_s = twist[0], twist[1]

        def first_stage(parts):
            turned = mm(one[...], jnp.concatenate(parts, axis=1).astype(BF16))
            out = []
            for c in range(len(parts)):
                real = turned[:half, c * LANES : (c + 1) * LANES]
                imag = turned[half:, c * LANES : (c + 1) * LANES]
                out.append(
                    jnp.concatenate(
                        [real * twist_c - imag * twist_s, -(imag * twist_c + real * twist_s)], axis=1
                    ).astype(BF16)
                )
            return jnp.concatenate(out, axis=0)

        drain(f_recv, rows - 2, a2a_recv.at[0])
        got = [f_recv[:, c].astype(F32) for c in range(per)]
        plus = [x[:, :subs].reshape(half, LANES) for x in got]
        minus = [x[:, subs:].reshape(half, LANES) for x in got]
        spec_real = mm(first_stage(plus), two[:, :LANES])
        spec_imag = mm(first_stage(minus), two[:, LANES:])
        filters = []
        for c in range(per):
            energy = jnp.sum(plus[c] * plus[c] + minus[c] * minus[c], axis=0, keepdims=True)
            scale = lax.rsqrt(1.0 + 0.5 * jnp.sum(energy, axis=1, keepdims=True)) * (1.0 / (half * LANES))
            own = slice(c * half, (c + 1) * half)
            filters.append((spec_real[own] * scale, spec_imag[own] * scale))

        lane = lax.broadcasted_iota(jnp.int32, (half, LANES), 1)
        row = lax.broadcasted_iota(jnp.int32, (half, LANES), 0)
        channel = lax.broadcasted_iota(jnp.int32, (1, width), 1)

        def short_conv(x, which, c):
            left = pltpu.roll(x, 1, 1)
            left = jnp.where(lane == 0, pltpu.roll(left, 1, 0), left)
            left = jnp.where((lane == 0) & (row == 0), 0.0, left)
            right = pltpu.roll(x, LANES - 1, 1)
            right = jnp.where(lane == LANES - 1, pltpu.roll(right, half - 1, 0), right)
            right = jnp.where((lane == LANES - 1) & (row == half - 1), 0.0, right)
            tap = [
                jnp.sum(jnp.where(channel == per * me_r + c, taps[a, which : which + 1, :], 0.0), axis=1, keepdims=True)
                for a in range(3)
            ]
            return left * tap[0] + x * tap[1] + right * tap[2]

        drain(s_recv, rows - 1, a2a_recv.at[1])
        signals = []
        for c in range(per):
            raw = s_recv[:, c].astype(F32)
            signals.append(
                short_conv(raw[:, :subs].reshape(half, LANES), 1, c) * short_conv(raw[:, subs:].reshape(half, LANES), 2, c)
            )
        spec = mm(first_stage(signals), two[...])
        products = []
        for c in range(per):
            real, imag = spec[c * half : (c + 1) * half, :LANES], spec[c * half : (c + 1) * half, LANES:]
            f_real, f_imag = filters[c]
            products.append(
                jnp.concatenate([real * f_real - imag * f_imag, real * f_imag + imag * f_real], axis=1).astype(BF16)
            )
        back = mm(jnp.concatenate(products, axis=0), two_back[...])
        untwisted = []
        for c in range(per):
            real, imag = back[c * half : (c + 1) * half, :LANES], back[c * half : (c + 1) * half, LANES:]
            untwisted.append(
                jnp.concatenate(
                    [real * twist_c - imag * twist_s, imag * twist_c + real * twist_s], axis=0
                ).astype(BF16)
            )
        response = mm(one_back[...], jnp.concatenate(untwisted, axis=1))
        for c in range(per):
            y_send[:, c] = response[:, c * LANES : (c + 1) * LANES].reshape(rows, subs, LANES).astype(BF16)

        ring_z = rows // ring

        def response_peer(i, carry):
            peer = lax.rem(me_z + spread(lax.rem(i, ring_z), ring_z), ring_z) * ring + lax.rem(
                me_y + spread(i // ring_z, ring), ring
            )
            push(y_send.at[peer], y_recv.at[mine], 2, peer)
            return carry

        lax.fori_loop(0, rows - 1, response_peer, 0)
        y_recv[mine] = y_send[me_r]

    up.wait()
    down.wait()
    proj[7:8, :] = jnp.where(me_r == 0, 0.0, proj[7:8, :])
    proj[8 + length : 9 + length, :] = jnp.where(me_r == rows - 1, 0.0, proj[8 + length : 9 + length, :])
    tap = [
        jnp.concatenate([taps[a, 1:2, :], taps[a, 2:3, :], taps[a, 0:1, :]], axis=1) for a in range(3)
    ]
    conv = proj[7 : 7 + length, :] * tap[0] + proj[8 : 8 + length, :] * tap[1] + proj[9 : 9 + length, :] * tap[2]
    signal = (conv[:, :width] * conv[:, width : 2 * width]).astype(BF16).astype(F32)
    gate_s[...] = conv[:, 2 * width :].astype(BF16).astype(F32)
    sig_s[...] = skip[...] * signal
    late[7].wait()

    @pl.when(in_zone)
    def _():
        drain(y_recv, width - per, a2a_recv.at[2])

    @pl.when(me_r >= zone)
    def _():
        drain(y_recv, width, a2a_recv.at[2])

    replied = y_recv[...].astype(F32).reshape(width, length).T
    mixed = (gate_s[...] * (replied + sig_s[...])).astype(BF16)
    m_send[...] = mixed.reshape(cols, length // cols, width)

    def col_peer(i, carry):
        peer = lax.rem(me_c + spread(i, cols), cols)
        pltpu.make_async_remote_copy(
            m_send.at[peer], m_recv.at[me_c], a2a_send.at[3], a2a_recv.at[3],
            device_id=(me_r, peer), device_id_type=MESH,
        ).start()
        return carry

    lax.fori_loop(0, cols - 1, col_peer, 0)
    m_recv[me_c] = m_send[me_c]

    @pl.when(in_zone)
    def _():
        drain(s_send, width - per, a2a_send.at[1])
        drain(f_recv, rows - 2, a2a_send.at[0])
        drain(y_send, rows - 1, a2a_send.at[2])

    @pl.when(me_r >= zone)
    def _():
        drain(s_send, width, a2a_send.at[1])

    drain(m_recv, cols - 1, a2a_recv.at[3])
    whole = jnp.concatenate([m_recv[j] for j in range(cols)], axis=1)
    tile = min(512, out_ref.shape[1])
    for c in range(out_ref.shape[1] // tile):
        out_ref[:, c * tile : (c + 1) * tile] = mm(whole, out_w[:, c * tile : (c + 1) * tile]).astype(BF16)
    drain(m_send, cols - 1, a2a_send.at[3])


def on_device(rows, cols, *args):
    (
        tokens, outer_weight, inner_weight, value_weight, conv_taps, feature_weight, feature_phase, inner_mats,
        inner_phase, frequency, forward_weight, backward_weight, decay_rate, skip_gain, output_weight,
    ) = args
    length, model = tokens.shape
    width = outer_weight.shape[1]
    units = frequency.shape[0]
    subs = length // LANES
    seq_length = length * rows
    out_rows = length // cols
    operands = (
        tokens, outer_weight.T, inner_weight.T, value_weight.T, conv_taps, feature_weight, feature_phase.reshape(1, units),
        inner_mats, inner_phase, frequency.reshape(1, units), forward_weight.T, backward_weight.T,
        decay_rate.reshape(1, width), skip_gain.reshape(1, width), output_weight,
    ) + tables(rows * subs)
    per = width // (rows // 2)
    held = [
        ((length, model), BF16), ((3 * width, model), BF16), ((3, 3, width), F32), (feature_weight.shape, F32),
        ((1, units), F32), (inner_mats.shape, F32), (inner_phase.shape, F32), ((1, units), F32),
        ((2 * width, units), F32), ((1, width), F32), ((1, width), F32),
    ] + [(x.shape, x.dtype) for x in operands[14:]]
    scratch = [pltpu.VMEM(*x) for x in held] + [
        pltpu.VMEM((length + 16, 3 * width), F32),
        pltpu.VMEM((length, width), F32),
        pltpu.VMEM((length, width), F32),
        pltpu.VMEM((2, width, 2 * subs, LANES), BF16),
        pltpu.VMEM((rows, per, 2 * subs, LANES), BF16),
        pltpu.VMEM((width, 2 * subs, LANES), BF16),
        pltpu.VMEM((rows, per, 2 * subs, LANES), BF16),
        pltpu.VMEM((rows, per, subs, LANES), BF16),
        pltpu.VMEM((width, subs, LANES), BF16),
        pltpu.VMEM((cols, out_rows, width), BF16),
        pltpu.VMEM((cols, out_rows, width), BF16),
        pltpu.SemaphoreType.DMA((24,)),
        pltpu.SemaphoreType.DMA((2,)),
        pltpu.SemaphoreType.DMA((2,)),
        pltpu.SemaphoreType.DMA((4,)),
        pltpu.SemaphoreType.DMA((4,)),
    ]
    return pl.pallas_call(
        functools.partial(kernel, rows, cols, seq_length),
        out_shape=jax.ShapeDtypeStruct((out_rows, model), BF16),
        in_specs=[pl.BlockSpec(memory_space=pl.ANY)] * len(operands),
        out_specs=pl.BlockSpec(memory_space=pltpu.VMEM),
        scratch_shapes=scratch,
        compiler_params=pltpu.CompilerParams(
            collective_id=0, has_side_effects=True, vmem_limit_bytes=56 * 1024 * 1024
        ),
    )(*operands)


def solution(mesh):
    placed = (
        P("row", None),
        P(None, "col"),
        P(None, "col"),
        P(None, "col"),
        P(None, None, "col"),
        P(),
        P(),
        P(),
        P(),
        P(),
        P(None, "col"),
        P(None, "col"),
        P("col"),
        P("col"),
        P(),
    )
    return jax.shard_map(
        functools.partial(on_device, mesh.shape["row"], mesh.shape["col"]),
        mesh=mesh, in_specs=placed, out_specs=P(("row", "col"), None), check_vma=False,
    )
```

```python
import functools
import math

import jax
import jax.numpy as jnp
import numpy as np
from jax import lax
from jax.experimental import pallas as pl
from jax.experimental.pallas import tpu as pltpu
from jax.sharding import PartitionSpec as P

BANDS = 16
INNER = 2
LANES = 128
MESH = pl.DeviceIdType.MESH
F32 = jnp.float32
BF16 = jnp.bfloat16


def tables(row_blocks):
    total = 2 * row_blocks * LANES
    k = np.arange(row_blocks)
    r = np.arange(row_blocks)
    b = np.arange(LANES)
    outer = (np.outer(2 * k + 1, r) % (4 * row_blocks)) * (2.0 * math.pi / (4 * row_blocks))
    one = np.concatenate([np.cos(outer), np.sin(outer)], axis=0)
    one_back = np.concatenate([np.cos(outer).T, -np.sin(outer).T], axis=1)
    inner = (np.outer(b, b) % LANES) * (2.0 * math.pi / LANES)
    c, s = np.cos(inner), np.sin(inner)
    two = np.block([[c, -s], [s, c]])
    two_back = np.block([[c, s], [-s, c]])
    twist = np.outer(2 * k + 1, b) * (math.pi / total)
    return (
        jnp.asarray(one, BF16),
        jnp.asarray(one_back, BF16),
        jnp.asarray(two, BF16),
        jnp.asarray(two_back, BF16),
        jnp.asarray(np.stack([np.cos(twist), np.sin(twist)]), F32),
    )


def mm(a, b):
    return jnp.dot(a, b, preferred_element_type=F32)


def mm_t(a, b):
    return lax.dot_general(a, b, (((1,), (1,)), ((), ())), preferred_element_type=F32)


def split(x):
    high = x.astype(BF16)
    return high, (x - high.astype(F32)).astype(BF16)


TURN = 2.0 * math.pi


def sine_turns(x):
    x = jnp.maximum(jnp.minimum(x, 0.5 - x), -0.5 - x)
    y = x * x
    p = y * (2.6083159809786593e-6 * TURN**9) - 1.9810690719168633e-4 * TURN**7
    p = p * y + 8.333078585565090e-3 * TURN**5
    p = p * y - 1.6666659712791443e-1 * TURN**3
    return x * (p * y + TURN)


def sine(x):
    return sine_turns(x - jnp.round(x))


def kernel(rows, cols, seq_length, *refs):
    (
        tokens, outer_w, inner_w, value_w, taps_h, first_h, phase_h, mats_h, iphase_h, freq_h,
        ahead_h, behind_h, rate_h, skip_h, map_h, one_h, one_back_h, two_h, two_back_h, twist_h,
        out_ref,
        tok, w_all, taps, first, phase, mats, iphase, freq, both, rate, skip,
        out_w, one, one_back, two, two_back, twist,
        proj, gate_s, sig_s, f_send, f_recv, s_send, s_recv, y_send, y_recv, m_send, m_recv,
        load_sem, halo_send, halo_recv, a2a_send, a2a_recv, hello,
    ) = refs
    me_r, me_c = lax.axis_index("row"), lax.axis_index("col")
    length = tok.shape[0]
    width = w_all.shape[0] // 3
    subs = length // LANES
    zone = rows // 2
    per = width // zone
    ring = 8 if rows % 8 == 0 else 2
    me_z, me_y = me_r // ring, lax.rem(me_r, ring)
    after, before = me_r + 1, me_r - 1
    in_zone = me_r < zone

    def load(src, dst, index):
        return pltpu.make_async_copy(src, dst, load_sem.at[index])

    small = [
        load(s, d, i)
        for i, (s, d) in enumerate(
            [
                (first_h, first), (phase_h, phase), (mats_h, mats), (iphase_h, iphase), (freq_h, freq),
                (ahead_h, both.at[pl.ds(0, width)]), (behind_h, both.at[pl.ds(width, width)]), (rate_h, rate),
            ]
        )
    ]
    weights = [load(w, w_all.at[pl.ds(i * width, width)], 8 + i) for i, w in enumerate((inner_w, value_w, outer_w))]
    depth = tok.shape[1]
    chunks = [(0, depth * 3 // 4), (depth * 3 // 4, depth // 4)]
    token_loads = [
        load(tokens.at[:, pl.ds(*c)], tok.at[:, pl.ds(*c)], 11 + i) for i, c in enumerate(chunks)
    ]

    @pl.when(in_zone)
    def _():
        for copy in small:
            copy.start()

    for copy in weights + token_loads:
        copy.start()

    barrier = pltpu.get_barrier_semaphore()

    def greet(row, col):
        pl.semaphore_signal(barrier, inc=1, device_id=(row, col), device_id_type=MESH)

    edge = jnp.zeros((8, proj.shape[1]), F32)
    proj[0:8, :] = edge
    proj[8 + length : 16 + length, :] = edge

    @pl.when(in_zone)
    def _():
        for d in range(1, zone):
            greet(lax.rem(me_r + d, zone), me_c)

    @pl.when(me_r >= zone)
    def _():
        greet(before, me_c)
        pl.when(me_r < rows - 1)(lambda: greet(after, me_c))

    me_x, core = me_c // 2, lax.rem(me_c, 2)
    chips = cols // 2
    far = chips // 2
    steps = [0] + [d for i in range(1, far + 1) for d in ([i] if 2 * i == chips else [i, chips - i])]

    def col_group(distance):
        if distance == 0:
            return [2 * me_x + 1 - core]
        return [2 * lax.rem(me_x + d, chips) + c for d in steps if min(d, chips - d) == distance for c in range(2)]

    def place_in_col(col):
        x = col // 2
        return 2 * (x + (x // max(far, 1)) * (chips + far - 1 - 2 * x)) + lax.rem(col, 2)

    my_place = place_in_col(me_c)
    col_peers = [peer for distance in range(far, -1, -1) for peer in col_group(distance)]
    for peer in col_peers:
        pl.when(my_place < place_in_col(peer))(functools.partial(greet, me_r, peer))

    def push(src, dst, index, row):
        pltpu.make_async_remote_copy(
            src, dst, a2a_send.at[index], a2a_recv.at[index], device_id=(row, me_c), device_id_type=MESH
        ).start()

    def drain(ref, count, sem):
        pltpu.make_async_copy(ref.at[pl.ds(0, count)], ref.at[pl.ds(0, count)], sem).wait()

    def enter():
        late_before = me_r // (zone + 1)
        late_after = (me_r + 1) // zone - 2 * ((me_r + 1) // rows)
        pl.semaphore_wait(barrier, zone - 1 + me_r // zone + late_before + late_after + my_place)

    mine = pl.ds(per * me_r, per)

    @pl.when(in_zone)
    def _():
        for copy in small:
            copy.wait()
        lane = lax.broadcasted_iota(jnp.int32, (length, LANES), 1)
        is_sine = lane > BANDS
        band = 1 + jnp.where(is_sine, lane - (BANDS + 1), lane - 1) * (seq_length // (4 * BANDS))
        shift = jnp.where(is_sine, seq_length, seq_length * 3 // 4)
        rates = jnp.broadcast_to(jnp.concatenate([rate[...], rate[...]], axis=1), (2 * width, 2 * width)).T[:, :1]
        behind = lax.broadcasted_iota(jnp.int32, (2 * width, length), 0) >= width
        pace = freq[...] * (1.0 / TURN)
        w_first, w_both = split(first[...] * pace), split(both[...])
        w_mats = [split(mats[level] * pace) for level in range(INNER)]

        def dot3(x, w, multiply):
            x_high, x_low = split(x)
            return multiply(x_high, w[0]) + (multiply(x_low, w[0]) + multiply(x_high, w[1]))

        for block in range(2):
            start = (me_r + block * zone) * length
            place = start + lax.broadcasted_iota(jnp.int32, (length, LANES), 0)
            turns = ((place * band + shift) & (seq_length - 1)) - seq_length // 2
            waves = sine_turns(turns.astype(F32) * (1.0 / seq_length))
            features = jnp.where(lane == 0, place.astype(F32) / (seq_length - 1), waves)[:, : 2 * BANDS + 1]
            hidden = sine(dot3(features, w_first, mm) + pace * phase[...])
            for level in range(INNER):
                hidden = sine(dot3(hidden, w_mats[level], mm) + pace * iphase[level : level + 1, :])
            turned = dot3(hidden, w_both, lambda h, w: mm_t(w, h))
            lag = start + lax.broadcasted_iota(jnp.int32, (2 * width, length), 1)
            turned = turned * jnp.exp(-(lag.astype(F32) / (seq_length - 1)) * rates)
            turned = jnp.where((lag == 0) & behind, 0.0, turned)
            fa, fb = turned[:width], turned[width:]
            f_send[block] = (
                jnp.concatenate([fa + fb, fa - fb], axis=1).reshape(width, 2 * subs, LANES).astype(BF16)
            )

        for row in range(zone, rows):
            greet(row, me_c)
        enter()

        def filter_peer(d, carry):
            peer = lax.rem(me_r + d, zone)
            push(f_send.at[0, pl.ds(per * peer, per)], f_recv.at[me_r], 0, peer)
            push(f_send.at[1, pl.ds(per * peer, per)], f_recv.at[me_r + zone], 0, peer)
            return carry

        lax.fori_loop(1, zone, filter_peer, 0)
        f_recv[me_r] = f_send[0, mine]
        f_recv[me_r + zone] = f_send[1, mine]

    for copy in weights:
        copy.wait()
    part = 0.0
    for (start, size), copy in zip(chunks, token_loads):
        copy.wait()
        own = slice(start, start + size)
        part = part + mm_t(tok[:, own], w_all[:, own])
    proj[pl.ds(8, length), :] = part.astype(BF16).astype(F32)
    turned = proj[pl.ds(8, length), : 2 * width].T
    s_send[...] = (
        jnp.concatenate([turned[:width], turned[width:]], axis=1).reshape(width, 2 * subs, LANES).astype(BF16)
    )

    @pl.when(me_r >= zone)
    def _():
        enter()

    zone_z = zone // ring
    near_y = [lax.rem(me_y + dy, ring) for dy in range(ring)]
    order = sorted(range(ring), key=lambda d: -min(d, ring - d))

    def signal_peer(peer):
        push(s_send.at[pl.ds(per * peer, per)], s_recv.at[me_r], 1, peer)

    for dy in order[:-1]:
        for z in range(zone_z):
            signal_peer(z * ring + near_y[dy])
    for z in range(zone_z):
        pl.when(me_z != z)(functools.partial(signal_peer, z * ring + me_y))

    @pl.when(in_zone)
    def _():
        s_recv[me_r] = s_send[mine]

    def answer(peer):
        pl.semaphore_signal(hello, inc=1, device_id=(me_r, peer), device_id_type=MESH)

    for peer in col_peers:
        pl.when(my_place > place_in_col(peer))(functools.partial(answer, peer))

    late = [
        load(s, d, 15 + i)
        for i, (s, d) in enumerate(
            [
                (taps_h, taps), (skip_h, skip), (one_h, one), (two_h, two), (twist_h, twist),
                (two_back_h, two_back), (one_back_h, one_back),
            ]
        )
    ]

    tall = 2 * width
    map_loads = [
        load(
            map_h.at[pl.ds(pl.multiple_of(tall * lax.rem(me_x + d, chips), tall), tall)],
            out_w.at[pl.ds(i * tall, tall)], 15 + len(late) + i,
        )
        for i, d in enumerate(steps)
    ]
    for copy in late + map_loads:
        copy.start()
    up = pltpu.make_async_remote_copy(
        proj.at[pl.ds(length, 8)], proj.at[pl.ds(0, 8)], halo_send.at[0], halo_recv.at[0],
        device_id=(after, me_c), device_id_type=MESH,
    )
    down = pltpu.make_async_remote_copy(
        proj.at[pl.ds(8, 8)], proj.at[pl.ds(8 + length, 8)], halo_send.at[1], halo_recv.at[1],
        device_id=(before, me_c), device_id_type=MESH,
    )
    pl.when(me_r < rows - 1)(up.start)
    pl.when(me_r > 0)(down.start)
    for copy in late:
        copy.wait()

    half = rows * subs
    @pl.when(in_zone)
    def _():
        twist_c, twist_s = twist[0], twist[1]

        def first_stage(parts):
            turned = mm(one[...], jnp.concatenate(parts, axis=1).astype(BF16))
            out = []
            for c in range(len(parts)):
                real = turned[:half, c * LANES : (c + 1) * LANES]
                imag = turned[half:, c * LANES : (c + 1) * LANES]
                out.append(
                    jnp.concatenate(
                        [real * twist_c - imag * twist_s, -(imag * twist_c + real * twist_s)], axis=1
                    ).astype(BF16)
                )
            return jnp.concatenate(out, axis=0)

        drain(f_recv, rows - 2, a2a_recv.at[0])
        got = [f_recv[:, c].astype(F32) for c in range(per)]
        plus = [x[:, :subs].reshape(half, LANES) for x in got]
        minus = [x[:, subs:].reshape(half, LANES) for x in got]
        spec_real = mm(first_stage(plus), two[:, :LANES])
        spec_imag = mm(first_stage(minus), two[:, LANES:])
        filters = []
        for c in range(per):
            energy = jnp.sum(plus[c] * plus[c] + minus[c] * minus[c], axis=0, keepdims=True)
            scale = lax.rsqrt(1.0 + 0.5 * jnp.sum(energy, axis=1, keepdims=True)) * (1.0 / (half * LANES))
            own = slice(c * half, (c + 1) * half)
            filters.append((spec_real[own] * scale, spec_imag[own] * scale))

        lane = lax.broadcasted_iota(jnp.int32, (half, LANES), 1)
        row = lax.broadcasted_iota(jnp.int32, (half, LANES), 0)
        channel = lax.broadcasted_iota(jnp.int32, (1, width), 1)

        def short_conv(x, which, c):
            left = pltpu.roll(x, 1, 1)
            left = jnp.where(lane == 0, pltpu.roll(left, 1, 0), left)
            left = jnp.where((lane == 0) & (row == 0), 0.0, left)
            right = pltpu.roll(x, LANES - 1, 1)
            right = jnp.where(lane == LANES - 1, pltpu.roll(right, half - 1, 0), right)
            right = jnp.where((lane == LANES - 1) & (row == half - 1), 0.0, right)
            tap = [
                jnp.sum(jnp.where(channel == per * me_r + c, taps[a, which : which + 1, :], 0.0), axis=1, keepdims=True)
                for a in range(3)
            ]
            return left * tap[0] + x * tap[1] + right * tap[2]

        drain(s_recv, rows - 1, a2a_recv.at[1])
        signals = []
        for c in range(per):
            raw = s_recv[:, c].astype(F32)
            signals.append(
                short_conv(raw[:, :subs].reshape(half, LANES), 1, c) * short_conv(raw[:, subs:].reshape(half, LANES), 2, c)
            )
        spec = mm(first_stage(signals), two[...])
        products = []
        for c in range(per):
            real, imag = spec[c * half : (c + 1) * half, :LANES], spec[c * half : (c + 1) * half, LANES:]
            f_real, f_imag = filters[c]
            products.append(
                jnp.concatenate([real * f_real - imag * f_imag, real * f_imag + imag * f_real], axis=1).astype(BF16)
            )
        back = mm(jnp.concatenate(products, axis=0), two_back[...])
        untwisted = []
        for c in range(per):
            real, imag = back[c * half : (c + 1) * half, :LANES], back[c * half : (c + 1) * half, LANES:]
            untwisted.append(
                jnp.concatenate(
                    [real * twist_c - imag * twist_s, imag * twist_c + real * twist_s], axis=0
                ).astype(BF16)
            )
        response = mm(one_back[...], jnp.concatenate(untwisted, axis=1))
        for c in range(per):
            y_send[:, c] = response[:, c * LANES : (c + 1) * LANES].reshape(rows, subs, LANES).astype(BF16)

        def response_peer(peer):
            push(y_send.at[peer], y_recv.at[mine], 2, peer)

        for dy in order:
            for z in range(zone_z, rows // ring):
                response_peer(z * ring + near_y[dy])
        for dy in order[:-1]:
            for z in range(zone_z):
                response_peer(z * ring + near_y[dy])
        for z in range(zone_z):
            pl.when(me_z != z)(functools.partial(response_peer, z * ring + me_y))
        y_recv[mine] = y_send[me_r]

    @pl.when(me_r < rows - 1)
    def _():
        up.wait_send()
        down.wait_recv()

    @pl.when(me_r > 0)
    def _():
        down.wait_send()
        up.wait_recv()

    tap = [
        jnp.concatenate([taps[a, 1:2, :], taps[a, 2:3, :], taps[a, 0:1, :]], axis=1) for a in range(3)
    ]
    conv = proj[7 : 7 + length, :] * tap[0] + proj[8 : 8 + length, :] * tap[1] + proj[9 : 9 + length, :] * tap[2]
    signal = (conv[:, :width] * conv[:, width : 2 * width]).astype(BF16).astype(F32)
    gate_s[...] = conv[:, 2 * width :].astype(BF16).astype(F32)
    sig_s[...] = skip[...] * signal
    for copy in map_loads:
        copy.wait()

    @pl.when(in_zone)
    def _():
        drain(y_recv, width - per, a2a_recv.at[2])

    @pl.when(me_r >= zone)
    def _():
        drain(y_recv, width, a2a_recv.at[2])

    replied = y_recv[...].astype(F32).reshape(width, length).T
    mixed = (gate_s[...] * (replied + sig_s[...])).astype(BF16)
    thin = length // cols // 2
    mixed = mixed.reshape(cols, 2, thin, width)
    m_send[...] = jnp.concatenate([mixed[:, 0], mixed[:, 1]], axis=2)

    pl.when(my_place < cols - 1)(lambda: pl.semaphore_wait(hello, cols - 1 - my_place))
    for distance in range(far, -1, -1):
        for peer in col_group(distance):
            pltpu.make_async_remote_copy(
                m_send.at[peer], m_recv.at[me_c], a2a_send.at[3], a2a_recv.at[3 + distance],
                device_id=(me_r, peer), device_id_type=MESH,
            ).start()
    m_recv[me_c] = m_send[me_c]

    @pl.when(in_zone)
    def _():
        drain(s_send, width - per, a2a_send.at[1])
        drain(f_recv, rows - 2, a2a_send.at[0])
        drain(y_send, rows - 1, a2a_send.at[2])

    @pl.when(me_r >= zone)
    def _():
        drain(s_send, width, a2a_send.at[1])

    total = None
    done = 0
    for group in [list(range(min(2, far + 1)))] + [[d] for d in range(2, far + 1)]:
        count = 0
        for distance in group:
            drain(m_recv, len(col_group(distance)), a2a_recv.at[3 + distance])
            count += sum(min(d, chips - d) == distance for d in steps)
        chosen = [lax.rem(me_x + d, chips) for d in steps[done : done + count]]
        slabs = [m_recv[2 * x + c] for x in chosen for c in range(2)]
        gathered = jnp.concatenate(
            [jnp.concatenate([slab[:, own] for slab in slabs], axis=1) for own in (slice(0, width), slice(width, tall))],
            axis=0,
        )
        term = mm(gathered, out_w[done * tall : (done + count) * tall, :])
        total = term if total is None else total + term
        done += count
    out_ref[...] = total.astype(BF16)
    drain(m_send, cols - 1, a2a_send.at[3])


def on_device(rows, cols, *args):
    (
        tokens, outer_weight, inner_weight, value_weight, conv_taps, feature_weight, feature_phase, inner_mats,
        inner_phase, frequency, forward_weight, backward_weight, decay_rate, skip_gain, output_weight,
    ) = args
    length, model = tokens.shape
    width = outer_weight.shape[1]
    units = frequency.shape[0]
    subs = length // LANES
    seq_length = length * rows
    out_rows = length // cols
    operands = (
        tokens, outer_weight.T, inner_weight.T, value_weight.T, conv_taps, feature_weight, feature_phase.reshape(1, units),
        inner_mats, inner_phase, frequency.reshape(1, units), forward_weight.T, backward_weight.T,
        decay_rate.reshape(1, width), skip_gain.reshape(1, width), output_weight,
    ) + tables(rows * subs)
    per = width // (rows // 2)
    held = [
        ((length, model), BF16), ((3 * width, model), BF16), ((3, 3, width), F32), (feature_weight.shape, F32),
        ((1, units), F32), (inner_mats.shape, F32), (inner_phase.shape, F32), ((1, units), F32),
        ((2 * width, units), F32), ((1, width), F32), ((1, width), F32),
    ] + [(x.shape, x.dtype) for x in operands[14:]]
    scratch = [pltpu.VMEM(*x) for x in held] + [
        pltpu.VMEM((length + 16, 3 * width), F32),
        pltpu.VMEM((length, width), F32),
        pltpu.VMEM((length, width), F32),
        pltpu.VMEM((2, width, 2 * subs, LANES), BF16),
        pltpu.VMEM((rows, per, 2 * subs, LANES), BF16),
        pltpu.VMEM((width, 2 * subs, LANES), BF16),
        pltpu.VMEM((rows, per, 2 * subs, LANES), BF16),
        pltpu.VMEM((rows, per, subs, LANES), BF16),
        pltpu.VMEM((width, subs, LANES), BF16),
        pltpu.VMEM((cols, out_rows // 2, 2 * width), BF16),
        pltpu.VMEM((cols, out_rows // 2, 2 * width), BF16),
        pltpu.SemaphoreType.DMA((32,)),
        pltpu.SemaphoreType.DMA((2,)),
        pltpu.SemaphoreType.DMA((2,)),
        pltpu.SemaphoreType.DMA((4,)),
        pltpu.SemaphoreType.DMA((4 + cols // 4,)),
        pltpu.SemaphoreType.REGULAR,
    ]
    return pl.pallas_call(
        functools.partial(kernel, rows, cols, seq_length),
        out_shape=pltpu.VMEM((out_rows, model), BF16),
        in_specs=[pl.BlockSpec(memory_space=pl.ANY)] * len(operands),
        out_specs=pl.BlockSpec(memory_space=pltpu.VMEM),
        scratch_shapes=scratch,
        compiler_params=pltpu.CompilerParams(
            collective_id=0, has_side_effects=True, vmem_limit_bytes=56 * 1024 * 1024
        ),
    )(*operands)


def solution(mesh):
    placed = (
        P("row", None),
        P(None, "col"),
        P(None, "col"),
        P(None, "col"),
        P(None, None, "col"),
        P(),
        P(),
        P(),
        P(),
        P(),
        P(None, "col"),
        P(None, "col"),
        P("col"),
        P("col"),
        P(),
    )
    return jax.shard_map(
        functools.partial(on_device, mesh.shape["row"], mesh.shape["col"]),
        mesh=mesh, in_specs=placed, out_specs=P(("row", "col"), None), check_vma=False,
    )
```

```python
import functools
import math

import jax
import jax.numpy as jnp
import numpy as np
from jax import lax
from jax.experimental import pallas as pl
from jax.experimental.pallas import tpu as pltpu
from jax.sharding import PartitionSpec as P

BANDS = 16
INNER = 2
LANES = 128
MESH = pl.DeviceIdType.MESH
F32 = jnp.float32
BF16 = jnp.bfloat16


def tables(row_blocks):
    total = 2 * row_blocks * LANES
    k = np.arange(row_blocks)
    r = np.arange(row_blocks)
    b = np.arange(LANES)
    outer = (np.outer(2 * k + 1, r) % (4 * row_blocks)) * (2.0 * math.pi / (4 * row_blocks))
    one = np.concatenate([np.cos(outer), np.sin(outer)], axis=0)
    one_back = np.concatenate([np.cos(outer).T, -np.sin(outer).T], axis=1)
    inner = (np.outer(b, b) % LANES) * (2.0 * math.pi / LANES)
    c, s = np.cos(inner), np.sin(inner)
    two = np.block([[c, -s], [s, c]])
    two_back = np.block([[c, s], [-s, c]])
    twist = np.outer(2 * k + 1, b) * (math.pi / total)
    return (
        jnp.asarray(one, BF16),
        jnp.asarray(one_back, BF16),
        jnp.asarray(two, BF16),
        jnp.asarray(two_back, BF16),
        jnp.asarray(np.stack([np.cos(twist), np.sin(twist)]), F32),
    )


def mm(a, b):
    return jnp.dot(a, b, preferred_element_type=F32)


def mm_t(a, b):
    return lax.dot_general(a, b, (((1,), (1,)), ((), ())), preferred_element_type=F32)


def split(x):
    high = x.astype(BF16)
    return high, (x - high.astype(F32)).astype(BF16)


TURN = 2.0 * math.pi


def sine_turns(x):
    x = jnp.maximum(jnp.minimum(x, 0.5 - x), -0.5 - x)
    y = x * x
    p = y * (2.6083159809786593e-6 * TURN**9) - 1.9810690719168633e-4 * TURN**7
    p = p * y + 8.333078585565090e-3 * TURN**5
    p = p * y - 1.6666659712791443e-1 * TURN**3
    return x * (p * y + TURN)


def sine(x):
    return sine_turns(x - jnp.round(x))


def kernel(rows, cols, seq_length, *refs):
    (
        tokens, outer_w, inner_w, value_w, taps_h, first_h, phase_h, mats_h, iphase_h, freq_h,
        ahead_h, behind_h, rate_h, skip_h, map_h, one_h, one_back_h, two_h, two_back_h, twist_h,
        out_ref,
        tok, w_all, taps, first, phase, mats, iphase, freq, both, rate, skip,
        out_w, one, one_back, two, two_back, twist,
        proj, gate_s, sig_s, f_send, f_recv, s_send, s_recv, y_send, y_recv, m_send, m_recv,
        load_sem, halo_send, halo_recv, a2a_send, a2a_recv, hello,
    ) = refs
    me_r, me_c = lax.axis_index("row"), lax.axis_index("col")
    length = tok.shape[0]
    width = w_all.shape[0] // 3
    subs = length // LANES
    zone = rows // 2
    per = width // zone
    ring = 8 if rows % 8 == 0 else 2
    me_z, me_y = me_r // ring, lax.rem(me_r, ring)
    after, before = me_r + 1, me_r - 1
    in_zone = me_r < zone
    zone_z = zone // ring
    near_y = [lax.rem(me_y + dy, ring) for dy in range(ring)]
    order = sorted(range(ring), key=lambda d: -min(d, ring - d))

    def load(src, dst, index):
        return pltpu.make_async_copy(src, dst, load_sem.at[index])

    small = [
        load(s, d, i)
        for i, (s, d) in enumerate(
            [
                (first_h, first), (phase_h, phase), (mats_h, mats), (iphase_h, iphase), (freq_h, freq),
                (ahead_h, both.at[pl.ds(0, width)]), (behind_h, both.at[pl.ds(width, width)]), (rate_h, rate),
            ]
        )
    ]
    weights = [load(w, w_all.at[pl.ds(i * width, width)], 8 + i) for i, w in enumerate((inner_w, value_w, outer_w))]
    high = length // 8
    token_loads = [load(tokens.at[pl.ds(i * high, high)], tok.at[pl.ds(i * high, high)], 11 + i) for i in range(8)]

    @pl.when(in_zone)
    def _():
        for copy in small:
            copy.start()

    for copy in weights + token_loads:
        copy.start()

    barrier = pltpu.get_barrier_semaphore()

    def greet(row, col):
        pl.semaphore_signal(barrier, inc=1, device_id=(row, col), device_id_type=MESH)

    edge = jnp.zeros((8, proj.shape[1]), F32)
    proj[0:8, :] = edge
    proj[8 + length : 16 + length, :] = edge

    @pl.when(in_zone)
    def _():
        for d in range(1, zone):
            greet(lax.rem(me_r + d, zone), me_c)

    def greet_late():
        for row in range(zone, rows):
            greet(row, me_c)

    pl.when(me_z == zone_z - 1)(greet_late)

    @pl.when(me_r >= zone)
    def _():
        greet(before, me_c)
        pl.when(me_r < rows - 1)(lambda: greet(after, me_c))

    me_x, core = me_c // 2, lax.rem(me_c, 2)
    chips = cols // 2
    far = chips // 2
    steps = [0] + [d for i in range(1, far + 1) for d in ([i] if 2 * i == chips else [i, chips - i])]

    def col_group(distance):
        if distance == 0:
            return [2 * me_x + 1 - core]
        return [2 * lax.rem(me_x + d, chips) + c for d in steps if min(d, chips - d) == distance for c in range(2)]

    def place_in_col(col):
        x = col // 2
        return 2 * (x + (x // max(far, 1)) * (chips + far - 1 - 2 * x)) + lax.rem(col, 2)

    my_place = place_in_col(me_c)
    col_peers = [peer for distance in range(far, -1, -1) for peer in col_group(distance)]
    for peer in col_peers:
        pl.when(my_place < place_in_col(peer))(functools.partial(greet, me_r, peer))

    def push(src, dst, index, row):
        pltpu.make_async_remote_copy(
            src, dst, a2a_send.at[index], a2a_recv.at[index], device_id=(row, me_c), device_id_type=MESH
        ).start()

    def drain(ref, count, sem):
        pltpu.make_async_copy(ref.at[pl.ds(0, count)], ref.at[pl.ds(0, count)], sem).wait()

    def enter():
        late_before = me_r // (zone + 1)
        late_after = (me_r + 1) // zone - 2 * ((me_r + 1) // rows)
        pl.semaphore_wait(barrier, zone - 1 + me_r // zone + late_before + late_after + my_place)

    mine = pl.ds(per * me_r, per)

    @pl.when(in_zone)
    def _():
        for copy in small:
            copy.wait()
        lane = lax.broadcasted_iota(jnp.int32, (length, LANES), 1)
        is_sine = lane > BANDS
        band = 1 + jnp.where(is_sine, lane - (BANDS + 1), lane - 1) * (seq_length // (4 * BANDS))
        shift = jnp.where(is_sine, seq_length, seq_length * 3 // 4)
        rates = jnp.broadcast_to(jnp.concatenate([rate[...], rate[...]], axis=1), (2 * width, 2 * width)).T[:, :1]
        behind = lax.broadcasted_iota(jnp.int32, (2 * width, length), 0) >= width
        pace = freq[...] * (1.0 / TURN)
        w_first, w_both = split(first[...] * pace), split(both[...])
        w_mats = [split(mats[level] * pace) for level in range(INNER)]

        def dot3(x, w, multiply):
            x_high, x_low = split(x)
            return multiply(x_high, w[0]) + (multiply(x_low, w[0]) + multiply(x_high, w[1]))

        for block in range(2):
            start = (me_r + block * zone) * length
            place = start + lax.broadcasted_iota(jnp.int32, (length, LANES), 0)
            turns = ((place * band + shift) & (seq_length - 1)) - seq_length // 2
            waves = sine_turns(turns.astype(F32) * (1.0 / seq_length))
            features = jnp.where(lane == 0, place.astype(F32) / (seq_length - 1), waves)[:, : 2 * BANDS + 1]
            hidden = sine(dot3(features, w_first, mm) + pace * phase[...])
            for level in range(INNER):
                hidden = sine(dot3(hidden, w_mats[level], mm) + pace * iphase[level : level + 1, :])
            turned = dot3(hidden, w_both, lambda h, w: mm_t(w, h))
            lag = start + lax.broadcasted_iota(jnp.int32, (2 * width, length), 1)
            turned = turned * jnp.exp(-(lag.astype(F32) / (seq_length - 1)) * rates)
            turned = jnp.where((lag == 0) & behind, 0.0, turned)
            fa, fb = turned[:width], turned[width:]
            f_send[block] = (
                jnp.concatenate([fa + fb, fa - fb], axis=1).reshape(width, 2 * subs, LANES).astype(BF16)
            )

        pl.when(me_z < zone_z - 1)(greet_late)
        enter()

        def filter_peer(peer):
            push(f_send.at[0, pl.ds(per * peer, per)], f_recv.at[me_r], 0, peer)
            push(f_send.at[1, pl.ds(per * peer, per)], f_recv.at[me_r + zone], 0, peer)

        for z in reversed(range(zone_z)):
            for dy in order[:-1]:
                filter_peer(z * ring + near_y[dy])
            pl.when(me_z != z)(functools.partial(filter_peer, z * ring + me_y))
        f_recv[me_r] = f_send[0, mine]
        f_recv[me_r + zone] = f_send[1, mine]

    for copy in weights:
        copy.wait()
    for copy in token_loads:
        copy.wait()
    proj[pl.ds(8, length), :] = mm_t(tok[...], w_all[...]).astype(BF16).astype(F32)
    turned = proj[pl.ds(8, length), : 2 * width].T
    s_send[...] = (
        jnp.concatenate([turned[:width], turned[width:]], axis=1).reshape(width, 2 * subs, LANES).astype(BF16)
    )

    @pl.when(me_r >= zone)
    def _():
        enter()


    def signal_peer(peer):
        push(s_send.at[pl.ds(per * peer, per)], s_recv.at[me_r], 1, peer)

    for z in reversed(range(zone_z)):
        for dy in order[:-1]:
            signal_peer(z * ring + near_y[dy])
        pl.when(me_z != z)(functools.partial(signal_peer, z * ring + me_y))

    @pl.when(in_zone)
    def _():
        s_recv[me_r] = s_send[mine]

    def answer(peer):
        pl.semaphore_signal(hello, inc=1, device_id=(me_r, peer), device_id_type=MESH)

    for peer in col_peers:
        pl.when(my_place > place_in_col(peer))(functools.partial(answer, peer))

    late = [
        load(s, d, 19 + i)
        for i, (s, d) in enumerate(
            [
                (taps_h, taps), (skip_h, skip), (one_h, one), (two_h, two), (twist_h, twist),
                (two_back_h, two_back), (one_back_h, one_back),
            ]
        )
    ]

    tall = 2 * width
    map_loads = [
        load(
            map_h.at[pl.ds(pl.multiple_of(tall * lax.rem(me_x + d, chips), tall), tall)],
            out_w.at[pl.ds(i * tall, tall)], 19 + len(late) + i,
        )
        for i, d in enumerate(steps)
    ]
    for copy in late + map_loads:
        copy.start()
    up = pltpu.make_async_remote_copy(
        proj.at[pl.ds(length, 8)], proj.at[pl.ds(0, 8)], halo_send.at[0], halo_recv.at[0],
        device_id=(after, me_c), device_id_type=MESH,
    )
    down = pltpu.make_async_remote_copy(
        proj.at[pl.ds(8, 8)], proj.at[pl.ds(8 + length, 8)], halo_send.at[1], halo_recv.at[1],
        device_id=(before, me_c), device_id_type=MESH,
    )
    pl.when(me_r < rows - 1)(up.start)
    pl.when(me_r > 0)(down.start)
    for copy in late:
        copy.wait()

    half = rows * subs
    @pl.when(in_zone)
    def _():
        twist_c, twist_s = twist[0], twist[1]

        def first_stage(parts):
            turned = mm(one[...], jnp.concatenate(parts, axis=1).astype(BF16))
            out = []
            for c in range(len(parts)):
                real = turned[:half, c * LANES : (c + 1) * LANES]
                imag = turned[half:, c * LANES : (c + 1) * LANES]
                out.append(
                    jnp.concatenate(
                        [real * twist_c - imag * twist_s, -(imag * twist_c + real * twist_s)], axis=1
                    ).astype(BF16)
                )
            return jnp.concatenate(out, axis=0)

        drain(f_recv, rows - 2, a2a_recv.at[0])
        got = [f_recv[:, c].astype(F32) for c in range(per)]
        plus = [x[:, :subs].reshape(half, LANES) for x in got]
        minus = [x[:, subs:].reshape(half, LANES) for x in got]
        spec_real = mm(first_stage(plus), two[:, :LANES])
        spec_imag = mm(first_stage(minus), two[:, LANES:])
        filters = []
        for c in range(per):
            energy = jnp.sum(plus[c] * plus[c] + minus[c] * minus[c], axis=0, keepdims=True)
            scale = lax.rsqrt(1.0 + 0.5 * jnp.sum(energy, axis=1, keepdims=True)) * (1.0 / (half * LANES))
            own = slice(c * half, (c + 1) * half)
            filters.append((spec_real[own] * scale, spec_imag[own] * scale))

        lane = lax.broadcasted_iota(jnp.int32, (half, LANES), 1)
        row = lax.broadcasted_iota(jnp.int32, (half, LANES), 0)
        channel = lax.broadcasted_iota(jnp.int32, (1, width), 1)

        def short_conv(x, which, c):
            left = pltpu.roll(x, 1, 1)
            left = jnp.where(lane == 0, pltpu.roll(left, 1, 0), left)
            left = jnp.where((lane == 0) & (row == 0), 0.0, left)
            right = pltpu.roll(x, LANES - 1, 1)
            right = jnp.where(lane == LANES - 1, pltpu.roll(right, half - 1, 0), right)
            right = jnp.where((lane == LANES - 1) & (row == half - 1), 0.0, right)
            tap = [
                jnp.sum(jnp.where(channel == per * me_r + c, taps[a, which : which + 1, :], 0.0), axis=1, keepdims=True)
                for a in range(3)
            ]
            return left * tap[0] + x * tap[1] + right * tap[2]

        drain(s_recv, rows - 1, a2a_recv.at[1])
        signals = []
        for c in range(per):
            raw = s_recv[:, c].astype(F32)
            signals.append(
                short_conv(raw[:, :subs].reshape(half, LANES), 1, c) * short_conv(raw[:, subs:].reshape(half, LANES), 2, c)
            )
        spec = mm(first_stage(signals), two[...])
        products = []
        for c in range(per):
            real, imag = spec[c * half : (c + 1) * half, :LANES], spec[c * half : (c + 1) * half, LANES:]
            f_real, f_imag = filters[c]
            products.append(
                jnp.concatenate([real * f_real - imag * f_imag, real * f_imag + imag * f_real], axis=1).astype(BF16)
            )
        back = mm(jnp.concatenate(products, axis=0), two_back[...])
        untwisted = []
        for c in range(per):
            real, imag = back[c * half : (c + 1) * half, :LANES], back[c * half : (c + 1) * half, LANES:]
            untwisted.append(
                jnp.concatenate(
                    [real * twist_c - imag * twist_s, imag * twist_c + real * twist_s], axis=0
                ).astype(BF16)
            )
        response = mm(one_back[...], jnp.concatenate(untwisted, axis=1))
        for c in range(per):
            y_send[:, c] = response[:, c * LANES : (c + 1) * LANES].reshape(rows, subs, LANES).astype(BF16)

        def response_peer(peer):
            push(y_send.at[peer], y_recv.at[mine], 2, peer)

        for z in range(rows // ring):
            for dy in order[:-1]:
                response_peer(z * ring + near_y[dy])
            pl.when(me_z != z)(functools.partial(response_peer, z * ring + me_y))
        y_recv[mine] = y_send[me_r]

    @pl.when(me_r < rows - 1)
    def _():
        up.wait_send()
        down.wait_recv()

    @pl.when(me_r > 0)
    def _():
        down.wait_send()
        up.wait_recv()

    tap = [
        jnp.concatenate([taps[a, 1:2, :], taps[a, 2:3, :], taps[a, 0:1, :]], axis=1) for a in range(3)
    ]
    conv = proj[7 : 7 + length, :] * tap[0] + proj[8 : 8 + length, :] * tap[1] + proj[9 : 9 + length, :] * tap[2]
    signal = (conv[:, :width] * conv[:, width : 2 * width]).astype(BF16).astype(F32)
    gate_s[...] = conv[:, 2 * width :].astype(BF16).astype(F32)
    sig_s[...] = skip[...] * signal
    for copy in map_loads:
        copy.wait()

    @pl.when(in_zone)
    def _():
        drain(y_recv, width - per, a2a_recv.at[2])

    @pl.when(me_r >= zone)
    def _():
        drain(y_recv, width, a2a_recv.at[2])

    replied = y_recv[...].astype(F32).reshape(width, length).T
    mixed = (gate_s[...] * (replied + sig_s[...])).astype(BF16)
    thin = length // cols // 2
    mixed = mixed.reshape(cols, 2, thin, width)
    m_send[...] = jnp.concatenate([mixed[:, 0], mixed[:, 1]], axis=2)

    pl.when(my_place < cols - 1)(lambda: pl.semaphore_wait(hello, cols - 1 - my_place))
    for distance in range(far, -1, -1):
        for peer in col_group(distance):
            pltpu.make_async_remote_copy(
                m_send.at[peer], m_recv.at[me_c], a2a_send.at[3], a2a_recv.at[3 + distance],
                device_id=(me_r, peer), device_id_type=MESH,
            ).start()
    m_recv[me_c] = m_send[me_c]

    @pl.when(in_zone)
    def _():
        drain(s_send, width - per, a2a_send.at[1])
        drain(f_recv, rows - 2, a2a_send.at[0])
        drain(y_send, rows - 1, a2a_send.at[2])

    @pl.when(me_r >= zone)
    def _():
        drain(s_send, width, a2a_send.at[1])

    total = None
    done = 0
    for group in [list(range(min(2, far + 1)))] + [[d] for d in range(2, far + 1)]:
        count = 0
        for distance in group:
            drain(m_recv, len(col_group(distance)), a2a_recv.at[3 + distance])
            count += sum(min(d, chips - d) == distance for d in steps)
        chosen = [lax.rem(me_x + d, chips) for d in steps[done : done + count]]
        slabs = [m_recv[2 * x + c] for x in chosen for c in range(2)]
        gathered = jnp.concatenate(
            [jnp.concatenate([slab[:, own] for slab in slabs], axis=1) for own in (slice(0, width), slice(width, tall))],
            axis=0,
        )
        term = mm(gathered, out_w[done * tall : (done + count) * tall, :])
        total = term if total is None else total + term
        done += count
    out_ref[...] = total.astype(BF16)
    drain(m_send, cols - 1, a2a_send.at[3])


def on_device(rows, cols, *args):
    (
        tokens, outer_weight, inner_weight, value_weight, conv_taps, feature_weight, feature_phase, inner_mats,
        inner_phase, frequency, forward_weight, backward_weight, decay_rate, skip_gain, output_weight,
    ) = args
    length, model = tokens.shape
    width = outer_weight.shape[1]
    units = frequency.shape[0]
    subs = length // LANES
    seq_length = length * rows
    out_rows = length // cols
    operands = (
        tokens, outer_weight.T, inner_weight.T, value_weight.T, conv_taps, feature_weight, feature_phase.reshape(1, units),
        inner_mats, inner_phase, frequency.reshape(1, units), forward_weight.T, backward_weight.T,
        decay_rate.reshape(1, width), skip_gain.reshape(1, width), output_weight,
    ) + tables(rows * subs)
    per = width // (rows // 2)
    held = [
        ((length, model), BF16), ((3 * width, model), BF16), ((3, 3, width), F32), (feature_weight.shape, F32),
        ((1, units), F32), (inner_mats.shape, F32), (inner_phase.shape, F32), ((1, units), F32),
        ((2 * width, units), F32), ((1, width), F32), ((1, width), F32),
    ] + [(x.shape, x.dtype) for x in operands[14:]]
    scratch = [pltpu.VMEM(*x) for x in held] + [
        pltpu.VMEM((length + 16, 3 * width), F32),
        pltpu.VMEM((length, width), F32),
        pltpu.VMEM((length, width), F32),
        pltpu.VMEM((2, width, 2 * subs, LANES), BF16),
        pltpu.VMEM((rows, per, 2 * subs, LANES), BF16),
        pltpu.VMEM((width, 2 * subs, LANES), BF16),
        pltpu.VMEM((rows, per, 2 * subs, LANES), BF16),
        pltpu.VMEM((rows, per, subs, LANES), BF16),
        pltpu.VMEM((width, subs, LANES), BF16),
        pltpu.VMEM((cols, out_rows // 2, 2 * width), BF16),
        pltpu.VMEM((cols, out_rows // 2, 2 * width), BF16),
        pltpu.SemaphoreType.DMA((40,)),
        pltpu.SemaphoreType.DMA((2,)),
        pltpu.SemaphoreType.DMA((2,)),
        pltpu.SemaphoreType.DMA((4,)),
        pltpu.SemaphoreType.DMA((4 + cols // 4,)),
        pltpu.SemaphoreType.REGULAR,
    ]
    return pl.pallas_call(
        functools.partial(kernel, rows, cols, seq_length),
        out_shape=pltpu.VMEM((out_rows, model), BF16),
        in_specs=[pl.BlockSpec(memory_space=pl.ANY)] * len(operands),
        out_specs=pl.BlockSpec(memory_space=pltpu.VMEM),
        scratch_shapes=scratch,
        compiler_params=pltpu.CompilerParams(
            collective_id=0, has_side_effects=True, vmem_limit_bytes=56 * 1024 * 1024
        ),
    )(*operands)


def solution(mesh):
    placed = (
        P("row", None),
        P(None, "col"),
        P(None, "col"),
        P(None, "col"),
        P(None, None, "col"),
        P(),
        P(),
        P(),
        P(),
        P(),
        P(None, "col"),
        P(None, "col"),
        P("col"),
        P("col"),
        P(),
    )
    return jax.shard_map(
        functools.partial(on_device, mesh.shape["row"], mesh.shape["col"]),
        mesh=mesh, in_specs=placed, out_specs=P(("row", "col"), None), check_vma=False,
    )
```

```python
import functools
import math

import jax
import jax.numpy as jnp
import numpy as np
from jax import lax
from jax.experimental import pallas as pl
from jax.experimental.pallas import tpu as pltpu
from jax.sharding import PartitionSpec as P

BANDS = 16
INNER = 2
LANES = 128
MESH = pl.DeviceIdType.MESH
F32 = jnp.float32
BF16 = jnp.bfloat16


def tables(row_blocks):
    total = 2 * row_blocks * LANES
    k = np.arange(row_blocks)
    r = np.arange(row_blocks)
    b = np.arange(LANES)
    outer = (np.outer(2 * k + 1, r) % (4 * row_blocks)) * (2.0 * math.pi / (4 * row_blocks))
    one = np.concatenate([np.cos(outer), np.sin(outer)], axis=0)
    one_back = np.concatenate([np.cos(outer).T, -np.sin(outer).T], axis=1)
    inner = (np.outer(b, b) % LANES) * (2.0 * math.pi / LANES)
    c, s = np.cos(inner), np.sin(inner)
    two = np.block([[c, -s], [s, c]])
    two_back = np.block([[c, s], [-s, c]])
    twist = np.outer(2 * k + 1, b) * (math.pi / total)
    return (
        jnp.asarray(one, BF16),
        jnp.asarray(one_back, BF16),
        jnp.asarray(two, BF16),
        jnp.asarray(two_back, BF16),
        jnp.asarray(np.stack([np.cos(twist), np.sin(twist)]), F32),
    )


def mm(a, b):
    return jnp.dot(a, b, preferred_element_type=F32)


def mm_t(a, b):
    return lax.dot_general(a, b, (((1,), (1,)), ((), ())), preferred_element_type=F32)


def split(x):
    high = x.astype(BF16)
    return high, (x - high.astype(F32)).astype(BF16)


TURN = 2.0 * math.pi


def sine_turns(x):
    x = jnp.maximum(jnp.minimum(x, 0.5 - x), -0.5 - x)
    y = x * x
    p = y * (2.6083159809786593e-6 * TURN**9) - 1.9810690719168633e-4 * TURN**7
    p = p * y + 8.333078585565090e-3 * TURN**5
    p = p * y - 1.6666659712791443e-1 * TURN**3
    return x * (p * y + TURN)


def sine(x):
    return sine_turns(x - jnp.round(x))


def kernel(rows, cols, seq_length, *refs):
    (
        tokens, outer_w, inner_w, value_w, taps_h, first_h, phase_h, mats_h, iphase_h, freq_h,
        ahead_h, behind_h, rate_h, skip_h, map_h, one_h, one_back_h, two_h, two_back_h, twist_h,
        out_ref,
        tok, w_all, taps, first, phase, mats, iphase, freq, both, rate, skip,
        out_w, one, one_back, two, two_back, twist,
        proj, gate_s, sig_s, f_send, f_recv, s_send, s_recv, y_send, y_recv, m_send, m_recv,
        load_sem, halo_send, halo_recv, a2a_send, a2a_recv, hello,
    ) = refs
    me_r, me_c = lax.axis_index("row"), lax.axis_index("col")
    length = tok.shape[0]
    width = w_all.shape[0] // 3
    subs = length // LANES
    zone = rows // 2
    per = width // zone
    ring = 8 if rows % 8 == 0 else 2
    me_z, me_y = me_r // ring, lax.rem(me_r, ring)
    after, before = me_r + 1, me_r - 1
    in_zone = me_r < zone
    zone_z = zone // ring
    near_y = [lax.rem(me_y + dy, ring) for dy in range(ring)]
    order = sorted(range(ring), key=lambda d: -min(d, ring - d))

    def load(src, dst, index):
        return pltpu.make_async_copy(src, dst, load_sem.at[index])

    small = [
        load(s, d, i)
        for i, (s, d) in enumerate(
            [
                (first_h, first), (phase_h, phase), (mats_h, mats), (iphase_h, iphase), (freq_h, freq),
                (ahead_h, both.at[pl.ds(0, width)]), (behind_h, both.at[pl.ds(width, width)]), (rate_h, rate),
            ]
        )
    ]
    weights = [load(w, w_all.at[pl.ds(i * width, width)], 8 + i) for i, w in enumerate((inner_w, value_w, outer_w))]
    high = length // 8
    token_loads = [load(tokens.at[pl.ds(i * high, high)], tok.at[pl.ds(i * high, high)], 11 + i) for i in range(8)]

    @pl.when(in_zone)
    def _():
        for copy in small:
            copy.start()

    for copy in weights + token_loads:
        copy.start()

    barrier = pltpu.get_barrier_semaphore()

    def greet(row, col):
        pl.semaphore_signal(barrier, inc=1, device_id=(row, col), device_id_type=MESH)

    edge = jnp.zeros((8, proj.shape[1]), F32)
    proj[0:8, :] = edge
    proj[8 + length : 16 + length, :] = edge

    @pl.when(in_zone)
    def _():
        for d in range(1, zone):
            greet(lax.rem(me_r + d, zone), me_c)

    def greet_late():
        for row in range(zone, rows):
            greet(row, me_c)

    pl.when(me_z == zone_z - 1)(greet_late)

    @pl.when(me_r >= zone)
    def _():
        greet(before, me_c)
        pl.when(me_r < rows - 1)(lambda: greet(after, me_c))

    me_x, core = me_c // 2, lax.rem(me_c, 2)
    chips = cols // 2
    far = chips // 2
    steps = [0] + [d for i in range(1, far + 1) for d in ([i] if 2 * i == chips else [i, chips - i])]

    def col_group(distance):
        if distance == 0:
            return [2 * me_x + 1 - core]
        return [2 * lax.rem(me_x + d, chips) + c for d in steps if min(d, chips - d) == distance for c in range(2)]

    def place_in_col(col):
        x = col // 2
        return 2 * (x + (x // max(far, 1)) * (chips + far - 1 - 2 * x)) + lax.rem(col, 2)

    my_place = place_in_col(me_c)
    col_peers = [peer for distance in range(far, -1, -1) for peer in col_group(distance)]
    for peer in col_peers:
        pl.when(my_place < place_in_col(peer))(functools.partial(greet, me_r, peer))

    def push(src, dst, index, row):
        pltpu.make_async_remote_copy(
            src, dst, a2a_send.at[index], a2a_recv.at[index], device_id=(row, me_c), device_id_type=MESH
        ).start()

    def drain(ref, count, sem):
        pltpu.make_async_copy(ref.at[pl.ds(0, count)], ref.at[pl.ds(0, count)], sem).wait()

    def enter():
        late_before = me_r // (zone + 1)
        late_after = (me_r + 1) // zone - 2 * ((me_r + 1) // rows)
        pl.semaphore_wait(barrier, zone - 1 + me_r // zone + late_before + late_after + my_place)

    mine = pl.ds(per * me_r, per)

    @pl.when(in_zone)
    def _():
        for copy in small:
            copy.wait()
        lane = lax.broadcasted_iota(jnp.int32, (length, LANES), 1)
        is_sine = lane > BANDS
        band = 1 + jnp.where(is_sine, lane - (BANDS + 1), lane - 1) * (seq_length // (4 * BANDS))
        shift = jnp.where(is_sine, seq_length, seq_length * 3 // 4)
        rates = jnp.broadcast_to(jnp.concatenate([rate[...], rate[...]], axis=1), (2 * width, 2 * width)).T[:, :1]
        behind = lax.broadcasted_iota(jnp.int32, (2 * width, length), 0) >= width
        pace = freq[...] * (1.0 / TURN)
        w_first, w_both = split(first[...] * pace), split(both[...])
        w_mats = [split(mats[level] * pace) for level in range(INNER)]

        def dot3(x, w, multiply):
            x_high, x_low = split(x)
            return multiply(x_high, w[0]) + (multiply(x_low, w[0]) + multiply(x_high, w[1]))

        for block in range(2):
            start = (me_r + block * zone) * length
            place = start + lax.broadcasted_iota(jnp.int32, (length, LANES), 0)
            turns = ((place * band + shift) & (seq_length - 1)) - seq_length // 2
            waves = sine_turns(turns.astype(F32) * (1.0 / seq_length))
            features = jnp.where(lane == 0, place.astype(F32) / (seq_length - 1), waves)[:, : 2 * BANDS + 1]
            hidden = sine(dot3(features, w_first, mm) + pace * phase[...])
            for level in range(INNER):
                hidden = sine(dot3(hidden, w_mats[level], mm) + pace * iphase[level : level + 1, :])
            turned = dot3(hidden, w_both, lambda h, w: mm_t(w, h))
            lag = start + lax.broadcasted_iota(jnp.int32, (2 * width, length), 1)
            turned = turned * jnp.exp(-(lag.astype(F32) / (seq_length - 1)) * rates)
            turned = jnp.where((lag == 0) & behind, 0.0, turned)
            fa, fb = turned[:width], turned[width:]
            f_send[block] = (
                jnp.concatenate([fa + fb, fa - fb], axis=1).reshape(width, 2 * subs, LANES).astype(BF16)
            )

        pl.when(me_z < zone_z - 1)(greet_late)
        enter()

        def filter_peer(peer):
            push(f_send.at[0, pl.ds(per * peer, per)], f_recv.at[me_r], 0, peer)
            push(f_send.at[1, pl.ds(per * peer, per)], f_recv.at[me_r + zone], 0, peer)

        for z in reversed(range(zone_z)):
            for dy in order[:-1]:
                filter_peer(z * ring + near_y[dy])
            pl.when(me_z != z)(functools.partial(filter_peer, z * ring + me_y))
        f_recv[me_r] = f_send[0, mine]
        f_recv[me_r + zone] = f_send[1, mine]

    for copy in weights:
        copy.wait()
    for copy in token_loads:
        copy.wait()
    proj[pl.ds(8, length), :] = mm_t(tok[...], w_all[...]).astype(BF16).astype(F32)
    turned = proj[pl.ds(8, length), : 2 * width].T
    s_send[...] = (
        jnp.concatenate([turned[:width], turned[width:]], axis=1).reshape(width, 2 * subs, LANES).astype(BF16)
    )

    @pl.when(me_r >= zone)
    def _():
        enter()


    def signal_peer(peer):
        push(s_send.at[pl.ds(per * peer, per)], s_recv.at[me_r], 1, peer)

    for z in reversed(range(zone_z)):
        for dy in order[:-1]:
            signal_peer(z * ring + near_y[dy])
        pl.when(me_z != z)(functools.partial(signal_peer, z * ring + me_y))

    @pl.when(in_zone)
    def _():
        s_recv[me_r] = s_send[mine]

    def answer(peer):
        pl.semaphore_signal(hello, inc=1, device_id=(me_r, peer), device_id_type=MESH)

    for peer in col_peers:
        pl.when(my_place > place_in_col(peer))(functools.partial(answer, peer))

    late = [
        load(s, d, 19 + i)
        for i, (s, d) in enumerate(
            [
                (taps_h, taps), (skip_h, skip), (one_h, one), (two_h, two), (twist_h, twist),
                (two_back_h, two_back), (one_back_h, one_back),
            ]
        )
    ]

    tall = 2 * width
    map_loads = [
        load(
            map_h.at[pl.ds(pl.multiple_of(tall * lax.rem(me_x + d, chips), tall), tall)],
            out_w.at[pl.ds(i * tall, tall)], 19 + len(late) + i,
        )
        for i, d in enumerate(steps)
    ]
    for copy in late + map_loads:
        copy.start()
    up = pltpu.make_async_remote_copy(
        proj.at[pl.ds(length, 8)], proj.at[pl.ds(0, 8)], halo_send.at[0], halo_recv.at[0],
        device_id=(after, me_c), device_id_type=MESH,
    )
    down = pltpu.make_async_remote_copy(
        proj.at[pl.ds(8, 8)], proj.at[pl.ds(8 + length, 8)], halo_send.at[1], halo_recv.at[1],
        device_id=(before, me_c), device_id_type=MESH,
    )
    pl.when(me_r < rows - 1)(up.start)
    pl.when(me_r > 0)(down.start)
    for copy in late:
        copy.wait()

    half = rows * subs
    @pl.when(in_zone)
    def _():
        twist_c, twist_s = twist[0], twist[1]

        def first_stage(parts):
            turned = mm(one[...], jnp.concatenate(parts, axis=1).astype(BF16))
            out = []
            for c in range(len(parts)):
                real = turned[:half, c * LANES : (c + 1) * LANES]
                imag = turned[half:, c * LANES : (c + 1) * LANES]
                out.append(
                    jnp.concatenate(
                        [real * twist_c - imag * twist_s, -(imag * twist_c + real * twist_s)], axis=1
                    ).astype(BF16)
                )
            return jnp.concatenate(out, axis=0)

        drain(f_recv, rows - 2, a2a_recv.at[0])
        got = [f_recv[:, c].astype(F32) for c in range(per)]
        plus = [x[:, :subs].reshape(half, LANES) for x in got]
        minus = [x[:, subs:].reshape(half, LANES) for x in got]
        spec_real = mm(first_stage(plus), two[:, :LANES])
        spec_imag = mm(first_stage(minus), two[:, LANES:])
        filters = []
        for c in range(per):
            energy = jnp.sum(plus[c] * plus[c] + minus[c] * minus[c], axis=0, keepdims=True)
            scale = lax.rsqrt(1.0 + 0.5 * jnp.sum(energy, axis=1, keepdims=True)) * (1.0 / (half * LANES))
            own = slice(c * half, (c + 1) * half)
            filters.append((spec_real[own] * scale, spec_imag[own] * scale))

        lane = lax.broadcasted_iota(jnp.int32, (half, LANES), 1)
        row = lax.broadcasted_iota(jnp.int32, (half, LANES), 0)
        channel = lax.broadcasted_iota(jnp.int32, (1, width), 1)

        own_taps = {
            (which, c): [
                jnp.sum(jnp.where(channel == per * me_r + c, taps[a, which : which + 1, :], 0.0), axis=1, keepdims=True)
                for a in range(3)
            ]
            for which in (1, 2)
            for c in range(per)
        }

        def short_conv(x, which, c):
            tap = own_taps[which, c]
            left = pltpu.roll(x, 1, 1)
            left = jnp.where(lane == 0, pltpu.roll(left, 1, 0), left)
            left = jnp.where((lane == 0) & (row == 0), 0.0, left)
            right = pltpu.roll(x, LANES - 1, 1)
            right = jnp.where(lane == LANES - 1, pltpu.roll(right, half - 1, 0), right)
            right = jnp.where((lane == LANES - 1) & (row == half - 1), 0.0, right)
            return left * tap[0] + x * tap[1] + right * tap[2]

        drain(s_recv, rows - 1, a2a_recv.at[1])
        signals = []
        for c in range(per):
            raw = s_recv[:, c].astype(F32)
            signals.append(
                short_conv(raw[:, :subs].reshape(half, LANES), 1, c) * short_conv(raw[:, subs:].reshape(half, LANES), 2, c)
            )
        spec = mm(first_stage(signals), two[...])
        products = []
        for c in range(per):
            real, imag = spec[c * half : (c + 1) * half, :LANES], spec[c * half : (c + 1) * half, LANES:]
            f_real, f_imag = filters[c]
            products.append(
                jnp.concatenate([real * f_real - imag * f_imag, real * f_imag + imag * f_real], axis=1).astype(BF16)
            )
        back = mm(jnp.concatenate(products, axis=0), two_back[...])
        untwisted = []
        for c in range(per):
            real, imag = back[c * half : (c + 1) * half, :LANES], back[c * half : (c + 1) * half, LANES:]
            untwisted.append(
                jnp.concatenate(
                    [real * twist_c - imag * twist_s, imag * twist_c + real * twist_s], axis=0
                ).astype(BF16)
            )
        response = mm(one_back[...], jnp.concatenate(untwisted, axis=1))
        for c in range(per):
            y_send[:, c] = response[:, c * LANES : (c + 1) * LANES].reshape(rows, subs, LANES).astype(BF16)

        def response_peer(peer):
            push(y_send.at[peer], y_recv.at[mine], 2, peer)

        for z in range(rows // ring):
            for dy in order[:-1]:
                response_peer(z * ring + near_y[dy])
            pl.when(me_z != z)(functools.partial(response_peer, z * ring + me_y))
        y_recv[mine] = y_send[me_r]

    @pl.when(me_r < rows - 1)
    def _():
        up.wait_send()
        down.wait_recv()

    @pl.when(me_r > 0)
    def _():
        down.wait_send()
        up.wait_recv()

    tap = [
        jnp.concatenate([taps[a, 1:2, :], taps[a, 2:3, :], taps[a, 0:1, :]], axis=1) for a in range(3)
    ]
    conv = proj[7 : 7 + length, :] * tap[0] + proj[8 : 8 + length, :] * tap[1] + proj[9 : 9 + length, :] * tap[2]
    signal = (conv[:, :width] * conv[:, width : 2 * width]).astype(BF16).astype(F32)
    gate_s[...] = conv[:, 2 * width :].astype(BF16).astype(F32)
    sig_s[...] = skip[...] * signal
    for copy in map_loads:
        copy.wait()

    @pl.when(in_zone)
    def _():
        drain(y_recv, width - per, a2a_recv.at[2])

    @pl.when(me_r >= zone)
    def _():
        drain(y_recv, width, a2a_recv.at[2])

    replied = y_recv[...].astype(F32).reshape(width, length).T
    mixed = (gate_s[...] * (replied + sig_s[...])).astype(BF16)
    thin = length // cols // 2
    mixed = mixed.reshape(cols, 2, thin, width)
    m_send[...] = jnp.concatenate([mixed[:, 0], mixed[:, 1]], axis=2)

    pl.when(my_place < cols - 1)(lambda: pl.semaphore_wait(hello, cols - 1 - my_place))
    for distance in range(far, -1, -1):
        for peer in col_group(distance):
            pltpu.make_async_remote_copy(
                m_send.at[peer], m_recv.at[me_c], a2a_send.at[3], a2a_recv.at[3 + distance],
                device_id=(me_r, peer), device_id_type=MESH,
            ).start()
    m_recv[me_c] = m_send[me_c]

    @pl.when(in_zone)
    def _():
        drain(s_send, width - per, a2a_send.at[1])
        drain(f_recv, rows - 2, a2a_send.at[0])
        drain(y_send, rows - 1, a2a_send.at[2])

    @pl.when(me_r >= zone)
    def _():
        drain(s_send, width, a2a_send.at[1])

    total = None
    done = 0
    for group in [list(range(min(2, far + 1)))] + [[d] for d in range(2, far + 1)]:
        count = 0
        for distance in group:
            drain(m_recv, len(col_group(distance)), a2a_recv.at[3 + distance])
            count += sum(min(d, chips - d) == distance for d in steps)
        chosen = [lax.rem(me_x + d, chips) for d in steps[done : done + count]]
        slabs = [m_recv[2 * x + c] for x in chosen for c in range(2)]
        gathered = jnp.concatenate(
            [jnp.concatenate([slab[:, own] for slab in slabs], axis=1) for own in (slice(0, width), slice(width, tall))],
            axis=0,
        )
        term = mm(gathered, out_w[done * tall : (done + count) * tall, :])
        total = term if total is None else total + term
        done += count
    out_ref[...] = total.astype(BF16)
    drain(m_send, cols - 1, a2a_send.at[3])


def on_device(rows, cols, *args):
    (
        tokens, outer_weight, inner_weight, value_weight, conv_taps, feature_weight, feature_phase, inner_mats,
        inner_phase, frequency, forward_weight, backward_weight, decay_rate, skip_gain, output_weight,
    ) = args
    length, model = tokens.shape
    width = outer_weight.shape[1]
    units = frequency.shape[0]
    subs = length // LANES
    seq_length = length * rows
    out_rows = length // cols
    operands = (
        tokens, outer_weight.T, inner_weight.T, value_weight.T, conv_taps, feature_weight, feature_phase.reshape(1, units),
        inner_mats, inner_phase, frequency.reshape(1, units), forward_weight.T, backward_weight.T,
        decay_rate.reshape(1, width), skip_gain.reshape(1, width), output_weight,
    ) + tables(rows * subs)
    per = width // (rows // 2)
    held = [
        ((length, model), BF16), ((3 * width, model), BF16), ((3, 3, width), F32), (feature_weight.shape, F32),
        ((1, units), F32), (inner_mats.shape, F32), (inner_phase.shape, F32), ((1, units), F32),
        ((2 * width, units), F32), ((1, width), F32), ((1, width), F32),
    ] + [(x.shape, x.dtype) for x in operands[14:]]
    scratch = [pltpu.VMEM(*x) for x in held] + [
        pltpu.VMEM((length + 16, 3 * width), F32),
        pltpu.VMEM((length, width), F32),
        pltpu.VMEM((length, width), F32),
        pltpu.VMEM((2, width, 2 * subs, LANES), BF16),
        pltpu.VMEM((rows, per, 2 * subs, LANES), BF16),
        pltpu.VMEM((width, 2 * subs, LANES), BF16),
        pltpu.VMEM((rows, per, 2 * subs, LANES), BF16),
        pltpu.VMEM((rows, per, subs, LANES), BF16),
        pltpu.VMEM((width, subs, LANES), BF16),
        pltpu.VMEM((cols, out_rows // 2, 2 * width), BF16),
        pltpu.VMEM((cols, out_rows // 2, 2 * width), BF16),
        pltpu.SemaphoreType.DMA((40,)),
        pltpu.SemaphoreType.DMA((2,)),
        pltpu.SemaphoreType.DMA((2,)),
        pltpu.SemaphoreType.DMA((4,)),
        pltpu.SemaphoreType.DMA((4 + cols // 4,)),
        pltpu.SemaphoreType.REGULAR,
    ]
    return pl.pallas_call(
        functools.partial(kernel, rows, cols, seq_length),
        out_shape=pltpu.VMEM((out_rows, model), BF16),
        in_specs=[pl.BlockSpec(memory_space=pl.ANY)] * len(operands),
        out_specs=pl.BlockSpec(memory_space=pltpu.VMEM),
        scratch_shapes=scratch,
        compiler_params=pltpu.CompilerParams(
            collective_id=0, has_side_effects=True, vmem_limit_bytes=56 * 1024 * 1024
        ),
    )(*operands)


def solution(mesh):
    placed = (
        P("row", None),
        P(None, "col"),
        P(None, "col"),
        P(None, "col"),
        P(None, None, "col"),
        P(),
        P(),
        P(),
        P(),
        P(),
        P(None, "col"),
        P(None, "col"),
        P("col"),
        P("col"),
        P(),
    )
    return jax.shard_map(
        functools.partial(on_device, mesh.shape["row"], mesh.shape["col"]),
        mesh=mesh, in_specs=placed, out_specs=P(("row", "col"), None), check_vma=False,
    )
```
